512 devices in a mesh: sp: 128 (over z, x, core), tp: 4 (over y).
Axes of the slice: x: 4, y: 4, z: 16, core: 2. Of those that a mesh axis runs over, the one named last changes fastest.
Arguments:
- tokens: bfloat16 [24576, 2048], P(('sp', 'tp')), may hold values from -7 to 7
- input_norm_gain: float32 [2048], replicated, may hold values from 0.1 to 1.9
- paired_query_weight: bfloat16 [2048, 512], P('sp', 'tp'), may hold values from -16 to 16
- shared_key_weight: bfloat16 [2048, 64], replicated, may hold values from -1 to 1
- shared_value_weight: bfloat16 [2048, 64], replicated, may hold values from -0.125 to 0.125
- recurrent_query_weight: bfloat16 [2048, 1024], P('sp', 'tp'), may hold values from -0.125 to 0.125
- forget_gate_weight: bfloat16 [2048, 1024], P('sp', 'tp'), may hold values from -0.125 to 0.125
- recurrent_value_weight: bfloat16 [2048, 1024], P('sp', 'tp'), may hold values from -0.125 to 0.125
- attention_output_weight: bfloat16 [2048, 512], P('sp', 'tp'), may hold values from -0.15625 to 0.15625
- recurrent_output_weight: bfloat16 [2048, 1024], P('sp', 'tp'), may hold values from -0.15625 to 0.15625
- attention_head_gain: float32 [64], replicated, may hold values from 0.1 to 1.9
- recurrent_head_gain: float32 [128], replicated, may hold values from 0.1 to 1.9
- second_map_weight: float32 [8], P('tp'), may hold values from 0.3 to 0.8
- forget_leak_rate: float32 [1024], P('tp'), may hold values from 2e-05 to 0.05
- extra_log_decay: float32 [24576, 1024], P('sp', 'tp'), may hold values from -1 to 0
- initial_recurrent_state: float32 [8, 128, 128], P('tp'), may hold values from -0.12 to 0.12
Outputs:
- mixer_out: bfloat16 [24576, 2048], P(('sp', 'tp'))
The draws below stay inside these ranges and needn't reach their ends.
All inputs are finite; a program needn't handle non-finite values.
Results may differ from the reference program's by a relative error of at most 0.014.
Values may be sent and summed in bfloat16 or wider, within the bound.
No kernel may reach another device: no remote copies, remote signals or barrier semaphores. Data moves between devices by JAX's collectives and lax.ppermute only.
A program may use at most 128 MiB of HBM per device.

```python
import math
import jax
import jax.numpy as jnp
from jax import lax

D = 2048
DIFF_HEADS = 8
QK_DIM = 32
HEAD_DIM = 64
RECURRENT_HEADS = 8
RECURRENT_WIDTH = 128
REC_SPAN = 64
TOKEN_COUNT = 24576
N_TP = 4


def pair_raw(key):
    key_raw = jnp.clip(jax.random.normal(jax.random.fold_in(key, 101), (D, 2 * QK_DIM), jnp.float32), -4.0, 4.0)
    query_raw = jnp.clip(jax.random.normal(jax.random.fold_in(key, 102), (D, DIFF_HEADS * 2 * QK_DIM), jnp.float32), -4.0, 4.0)
    return (key_raw, query_raw)


def draw_shared_key_weight(key, part):
    key_raw, query_raw = pair_raw(key)
    return (key_raw * (2.0 / D) ** 0.5).astype(jnp.bfloat16)


def draw_paired_query_weight(key, part):
    key_raw, query_raw = pair_raw(key)
    weight_scale = (2.0 / D) ** 0.5
    return (query_raw * weight_scale).astype(jnp.bfloat16)


def draw_tokens(key, part):
    base_rows = jnp.clip(jax.random.normal(jax.random.fold_in(key, 201), (TOKEN_COUNT, D), jnp.float32), -6.0, 6.0)
    return base_rows.astype(jnp.bfloat16)


def draw_extra_log_decay(key, part):
    extra_decay_positions = jax.random.randint(jax.random.fold_in(key, 301), (8, RECURRENT_HEADS), 0, TOKEN_COUNT)
    row_position_index = jnp.arange(TOKEN_COUNT)
    extra_decay_flag = jnp.any(row_position_index[:, None, None] == extra_decay_positions[None], axis=1)
    extra_decay_depth = jax.random.uniform(jax.random.fold_in(key, 302), (TOKEN_COUNT, RECURRENT_HEADS), jnp.float32, jnp.log(0.5), jnp.log(0.8))
    extra_decay_field = jnp.where(extra_decay_flag, extra_decay_depth, 0.0)
    return jnp.repeat(extra_decay_field, RECURRENT_WIDTH, axis=1).astype(jnp.float32)


def block_scale(stream_key, extent, cuts, smallest, largest):
    factor_of, own = 1.0, jax.random.fold_in(stream_key, 6)
    for position, parts in cuts:
        heights = jnp.exp(jax.random.uniform(jax.random.fold_in(own, position), (parts,), jnp.float32, smallest / len(cuts), largest / len(cuts)))
        factor_of = factor_of * jnp.repeat(heights, extent[position] // parts).reshape([-1 if axis == position else 1 for axis in range(len(extent))])
    return factor_of


def centred(key, shape, deviation, reach, split=(), held_as=jnp.bfloat16):
    values = jax.random.normal(key, shape, jnp.float32) * deviation
    if len(split) > 0:
        values = block_scale(key, shape, split, -0.22, 0.18) * values
    return jnp.clip(values, min=-reach, max=reach).astype(held_as)


def setup_inputs(seed: int = 0) -> dict:
    seeds = jax.random.split(jax.random.key(seed), 17)
    return {
        "tokens": draw_tokens(jax.random.fold_in(seeds[16], 71), 0),
        "input_norm_gain": jnp.clip(1.0 + 0.18 * jax.random.normal(seeds[1], (D,), jnp.float32), 0.1, 1.9),
        "paired_query_weight": draw_paired_query_weight(jax.random.fold_in(seeds[16], 71), 0),
        "shared_key_weight": draw_shared_key_weight(jax.random.fold_in(seeds[16], 71), 0),
        "shared_value_weight": centred(seeds[4], (D, HEAD_DIM), D ** -0.5, 0.125),
        "recurrent_query_weight": centred(seeds[5], (D, RECURRENT_HEADS * RECURRENT_WIDTH), D ** -0.5, 0.125, ((0, 128), (1, 4))),
        "forget_gate_weight": centred(seeds[6], (D, RECURRENT_HEADS * RECURRENT_WIDTH), D ** -0.5, 0.125, ((0, 128), (1, 4))),
        "recurrent_value_weight": centred(seeds[7], (D, RECURRENT_HEADS * RECURRENT_WIDTH), D ** -0.5, 0.125, ((0, 128), (1, 4))),
        "attention_output_weight": centred(seeds[8], (D, DIFF_HEADS * HEAD_DIM), (DIFF_HEADS * HEAD_DIM + RECURRENT_HEADS * RECURRENT_WIDTH) ** -0.5, 0.15625, ((0, 128), (1, 4))),
        "recurrent_output_weight": centred(seeds[9], (D, RECURRENT_HEADS * RECURRENT_WIDTH), (DIFF_HEADS * HEAD_DIM + RECURRENT_HEADS * RECURRENT_WIDTH) ** -0.5, 0.15625, ((0, 128), (1, 4))),
        "attention_head_gain": jnp.clip(1.0 + 0.18 * jax.random.normal(seeds[10], (HEAD_DIM,), jnp.float32), 0.1, 1.9),
        "recurrent_head_gain": jnp.clip(1.0 + 0.18 * jax.random.normal(seeds[11], (RECURRENT_WIDTH,), jnp.float32), 0.1, 1.9),
        "second_map_weight": jnp.clip(0.3 + 0.5 * jax.random.uniform(seeds[12], (DIFF_HEADS,), jnp.float32) ** block_scale(seeds[12], (DIFF_HEADS,), ((0, 4),), -0.2, 0.2), 0.3, 0.8),
        "forget_leak_rate": jnp.clip(jnp.exp(math.log(0.05) - 7.824046 * jax.random.uniform(seeds[13], (RECURRENT_HEADS * RECURRENT_WIDTH,), jnp.float32) ** block_scale(seeds[13], (RECURRENT_HEADS * RECURRENT_WIDTH,), ((0, 4),), -0.2, 0.2)), 1.9999999494757503e-05, 0.05),
        "extra_log_decay": draw_extra_log_decay(jax.random.fold_in(seeds[16], 71), 0),
        "initial_recurrent_state": centred(seeds[15], (RECURRENT_HEADS, RECURRENT_WIDTH, RECURRENT_WIDTH), 0.02, 0.12, ((0, 4),), jnp.float32),
    }


epsilon = 1e-06

def rms_scale(matrix, gain):
    return matrix * lax.rsqrt(lax.optimization_barrier(jnp.mean(matrix * matrix, axis=-1, keepdims=True)) + epsilon) * gain

def project(normed, weight):
    return jnp.dot(normed, weight, preferred_element_type=jnp.float32).astype(jnp.bfloat16)

def widen(stored):
    return lax.optimization_barrier(stored).astype(jnp.float32)

def attend(queries, keys, values, second_map_weight, attention_head_gain):
    token_count = queries.shape[0]
    block_rows = math.gcd(token_count, 512)
    head_count = queries.shape[1] // (2 * QK_DIM)
    key_pair = keys.reshape(token_count, 2, QK_DIM)
    score_scale = 1.0 / math.sqrt(QK_DIM)

    def one_block(begin_row):
        query_rows = lax.dynamic_slice_in_dim(queries, begin_row, block_rows, 0).reshape(block_rows, head_count, 2, QK_DIM)
        head_outs = []
        for head_index in range(head_count):
            parts_list = []
            for component in range(2):
                scores = jnp.dot(query_rows[:, head_index, component], key_pair[:, component].T, preferred_element_type=jnp.float32) * score_scale
                peak_score = lax.optimization_barrier(jnp.max(scores, axis=1, keepdims=True))
                expo_terms = jnp.exp(scores - peak_score)
                totals = lax.optimization_barrier(jnp.sum(expo_terms, axis=1, keepdims=True))
                weighted = jnp.dot(expo_terms.astype(jnp.bfloat16), values, preferred_element_type=jnp.float32)
                parts_list.append(weighted / totals)
            blended = parts_list[0] - second_map_weight[head_index] * parts_list[1]
            head_outs.append(rms_scale(blended, attention_head_gain))
        return jnp.concatenate(head_outs, axis=1).astype(jnp.bfloat16)
    starts = jnp.arange(token_count // block_rows, dtype=jnp.int32) * block_rows
    pieces = lax.map(one_block, starts)
    return pieces.reshape(token_count, head_count * HEAD_DIM)

def recur_blocks(rec_query, inflow_state, rec_values, log_decay_values, initial):
    head_count, token_count, channel_width = rec_query.shape
    span_count = token_count // REC_SPAN

    def to_spans(matrix):
        return jnp.moveaxis(matrix.reshape(head_count, span_count, REC_SPAN, matrix.shape[-1]), 1, 0)
    lower_mask = jnp.tril(jnp.ones((REC_SPAN, REC_SPAN), jnp.float32))
    highest_precision = lax.Precision.HIGHEST

    def step(carried_state, inputs):
        query_span, inflow_span, value_segment, decay_span = inputs
        running = jnp.cumsum(decay_span, axis=1)
        segment_final = running[:, -1:, :]
        decayed_query = query_span * jnp.exp(running)
        inflow_dec = inflow_span * jnp.exp(-running)
        within_segment = jnp.einsum('hsk,htk->hst', decayed_query, inflow_dec, precision=highest_precision) * lower_mask
        segment_output = jnp.einsum('rcn,rni->rci', within_segment, value_segment, precision=highest_precision) + jnp.einsum('cwi,cip->cwp', decayed_query, carried_state, precision=highest_precision)
        inflow_final = inflow_span * jnp.exp(segment_final - running)
        carried_state = jnp.exp(segment_final)[:, 0, :, None] * carried_state + jnp.einsum('rgc,rgt->rct', inflow_final, value_segment, precision=highest_precision)
        return (carried_state, segment_output)
    final_state, span_outs = lax.scan(step, initial, (to_spans(rec_query), to_spans(inflow_state), to_spans(rec_values), to_spans(log_decay_values)))
    return jnp.moveaxis(span_outs, 0, 1).reshape(head_count, token_count, rec_values.shape[-1])

def reference(tokens, input_norm_gain, paired_query_weight, shared_key_weight, shared_value_weight, recurrent_query_weight, forget_gate_weight, recurrent_value_weight, attention_output_weight, recurrent_output_weight, attention_head_gain, recurrent_head_gain, second_map_weight, forget_leak_rate, extra_log_decay, initial_recurrent_state):
    token_count = tokens.shape[0]
    normed = rms_scale(tokens.astype(jnp.float32), input_norm_gain).astype(jnp.bfloat16)
    queries = project(normed, paired_query_weight)
    keys = project(normed, shared_key_weight)
    values = project(normed, shared_value_weight)
    attn_hidden = attend(queries, keys, values, second_map_weight, attention_head_gain)
    rec_query = jax.nn.silu(widen(project(normed, recurrent_query_weight)))
    gate_raw = widen(project(normed, forget_gate_weight))
    rec_values = widen(project(normed, recurrent_value_weight))
    inflow_state = forget_leak_rate * (1.0 - jax.nn.sigmoid(gate_raw))
    log_decay_values = jnp.log(1.0 - inflow_state) + extra_log_decay

    def heads_first(matrix):
        return matrix.reshape(token_count, RECURRENT_HEADS, RECURRENT_WIDTH).transpose(1, 0, 2)
    recurrent_output = recur_blocks(heads_first(rec_query), heads_first(inflow_state), heads_first(rec_values), heads_first(log_decay_values), initial_recurrent_state)
    rec_hidden = rms_scale(recurrent_output, recurrent_head_gain).transpose(1, 0, 2).reshape(token_count, RECURRENT_HEADS * RECURRENT_WIDTH)
    rec_hidden = rec_hidden.astype(jnp.bfloat16)
    attn_group = DIFF_HEADS * HEAD_DIM // N_TP
    rec_group = RECURRENT_HEADS * RECURRENT_WIDTH // N_TP
    summed = jnp.zeros((token_count, D), jnp.float32)
    for group_index in range(N_TP):
        attn_cols = slice(group_index * attn_group, (group_index + 1) * attn_group)
        rec_cols = slice(group_index * rec_group, (group_index + 1) * rec_group)
        group_part = jnp.dot(attn_hidden[:, attn_cols], attention_output_weight[:, attn_cols].T, preferred_element_type=jnp.float32) + jnp.dot(rec_hidden[:, rec_cols], recurrent_output_weight[:, rec_cols].T, preferred_element_type=jnp.float32)
        summed = summed + lax.optimization_barrier(group_part.astype(jnp.bfloat16)).astype(jnp.float32)
    return summed.astype(jnp.bfloat16)
```

```python
import functools
import math

import jax
import jax.numpy as jnp
from jax import lax
from jax.experimental import pallas as pl
from jax.experimental.pallas import tpu as pltpu
from jax.sharding import Mesh
from jax.sharding import PartitionSpec as P

QK_DIM = 32
HEAD_DIM = 64
RECURRENT_WIDTH = 128
REC_SPAN = 64
SP = ("z", "x", "c")
SP_TP = ("z", "x", "c", "tp")
KEY_BLOCK = 256
COLUMN_TILE = 256
PART_ROWS = 80

epsilon = 1e-06


def sent_to_all(x, axis):
    size = lax.axis_size(axis)
    return lax.all_to_all(jnp.broadcast_to(x[None], (size, *x.shape)), axis, 0, 0, tiled=True)


def rms_scale(matrix, gain):
    return matrix * lax.rsqrt(jnp.mean(matrix * matrix, axis=-1, keepdims=True) + epsilon) * gain


def project(normed, weight):
    return jnp.dot(normed, weight, preferred_element_type=jnp.float32).astype(jnp.bfloat16)


def whole(shape):
    return pl.BlockSpec(shape, lambda *_: (0,) * len(shape))


def dot_nt(a, b):
    return lax.dot_general(a, b, (((1,), (1,)), ((), ())), preferred_element_type=jnp.float32)


def dot_nn(a, b):
    return jnp.dot(a, b, preferred_element_type=jnp.float32)


def projection_kernel(rows_ref, normed_ref, query_ref, recur_ref, weight):
    n_c, n_x, n_z, rows = rows_ref.shape[:4]
    wide = weight.shape[1]
    for z in range(n_z):
        for x in range(n_x):
            for c in range(n_c):
                start = ((z * n_x + x) * n_c + c) * rows
                weight[start : start + rows, :] = rows_ref[c, x, z, :, :wide]
    normed = normed_ref[...]
    narrow = query_ref.shape[1]
    query_ref[...] = dot_nn(normed, weight[:, :narrow]).astype(jnp.bfloat16)
    step = 256
    for k in range(recur_ref.shape[1] // step):
        recur_ref[:, k * step : (k + 1) * step] = dot_nn(
            normed, weight[:, narrow + k * step : narrow + (k + 1) * step]
        ).astype(jnp.bfloat16)


def projections(gathered, normed, narrow, recur):
    tokens, width = normed.shape
    return pl.pallas_call(
        projection_kernel,
        grid=(1,),
        out_shape=(
            jax.ShapeDtypeStruct((tokens, narrow), jnp.bfloat16),
            jax.ShapeDtypeStruct((tokens, recur), jnp.bfloat16),
        ),
        in_specs=[whole(gathered.shape), whole(normed.shape)],
        out_specs=(whole((tokens, narrow)), whole((tokens, recur))),
        scratch_shapes=[pltpu.VMEM((width, narrow + recur), jnp.bfloat16)],
        cost_estimate=pl.CostEstimate(
            flops=2 * tokens * width * (narrow + recur),
            bytes_accessed=2 * width * (narrow + recur),
            transcendentals=0,
        ),
        name="projections",
    )(gathered, normed)


def one_hot(rows, cols, row_offset, col_offset, count):
    r = lax.broadcasted_iota(jnp.int32, (rows, cols), 0) - row_offset
    c = lax.broadcasted_iota(jnp.int32, (rows, cols), 1) - col_offset
    hit = (r == c) & (r >= 0) & (r < count)
    return jnp.where(hit, 1.0, 0.0).astype(jnp.bfloat16)


def attention_kernel(query_ref, *refs):
    key_value_refs, (out_ref, keys, values_t, lifted_q) = refs[:-4], refs[-4:]
    n_tp, tokens, _ = query_ref.shape
    n_c, n_x, n_z, rows, _ = key_value_refs[0].shape
    piece_rows = n_z * rows
    both = 2 * QK_DIM
    twice = one_hot(128, 128, 0, 0, both) + one_hot(128, 128, 0, both, both)
    pick_values = one_hot(PART_ROWS, 128, 0, both, HEAD_DIM)
    ones_row = jnp.where(
        lax.broadcasted_iota(jnp.int32, (PART_ROWS, piece_rows), 0) == HEAD_DIM, 1.0, 0.0
    )
    key_peak = jnp.zeros((8, 128), jnp.float32)
    index = 0
    for ref in key_value_refs:
        for c in range(n_c):
            for x in range(n_x):
                piece = ref[c, x].reshape(piece_rows, 128)
                at = index * piece_rows
                doubled = dot_nn(piece, twice)
                keys[at : at + piece_rows, :] = doubled.astype(jnp.bfloat16)
                size = jnp.abs(doubled).reshape(piece_rows // 8, 8, 128)
                key_peak = jnp.maximum(key_peak, jnp.max(size, axis=0))
                values_t[:, at : at + piece_rows] = (
                    dot_nt(pick_values, piece) + ones_row
                ).astype(jnp.bfloat16)
                index += 1
    key_count = index * piece_rows
    scale = math.log2(math.e) / math.sqrt(QK_DIM)
    lane = lax.broadcasted_iota(jnp.int32, (tokens, 128), 1) % both
    for tp in range(n_tp):
        scaled = query_ref[tp].astype(jnp.float32) * scale
        high = scaled.astype(jnp.bfloat16)
        low = (scaled - high.astype(jnp.float32)).astype(jnp.bfloat16)
        for head in range(2):
            spread = dot_nn(high, one_hot(128, 128, head * both, 0, both)) + dot_nn(
                low, one_hot(128, 128, head * both, both, both)
            )
            for part in range(2):
                own = (lane >= part * QK_DIM) & (lane < (part + 1) * QK_DIM)
                at = ((tp * 2 + head) * 2 + part) * tokens
                lifted_q[at : at + tokens, :] = jnp.where(own, spread, 0.0).astype(jnp.bfloat16)
    peak_row = jnp.max(key_peak, axis=0, keepdims=True) * 1.02
    bound = dot_nt(
        jnp.broadcast_to(peak_row, (8, 128)).astype(jnp.bfloat16), jnp.abs(lifted_q[...])
    )
    small = jnp.max(bound) < 100.0
    blocks = key_count // KEY_BLOCK
    tiles = lifted_q.shape[0] // COLUMN_TILE
    per_group = tiles // n_tp

    def store(tile, acc, shift):
        group, place = tile // per_group, tile % per_group
        at = pl.multiple_of(place * COLUMN_TILE, COLUMN_TILE)
        row = lax.broadcasted_iota(jnp.int32, (PART_ROWS - HEAD_DIM, COLUMN_TILE), 0)
        tail = jnp.zeros(row.shape, jnp.float32)
        slot = 0
        for rest in (acc[HEAD_DIM : HEAD_DIM + 1, :], shift):
            for _ in range(3):
                high = rest.astype(jnp.bfloat16).astype(jnp.float32)
                tail = jnp.where(row == slot, high, tail)
                rest = rest - high
                slot += 1
        out_ref[group, :HEAD_DIM, pl.ds(at, COLUMN_TILE)] = acc[:HEAD_DIM, :].astype(jnp.bfloat16)
        out_ref[group, HEAD_DIM:, pl.ds(at, COLUMN_TILE)] = tail.astype(jnp.bfloat16)

    @pl.when(small)
    def _():
        @pl.loop(0, tiles)
        def _(tile):
            start = pl.multiple_of(tile * COLUMN_TILE, COLUMN_TILE)
            q = lifted_q[pl.ds(start, COLUMN_TILE), :]
            acc = jnp.zeros((PART_ROWS, COLUMN_TILE), jnp.float32)
            for b in range(blocks):
                span = slice(b * KEY_BLOCK, (b + 1) * KEY_BLOCK)
                scores = dot_nt(keys[span, :], q)
                acc = acc + dot_nn(values_t[:, span], jnp.exp2(scores).astype(jnp.bfloat16))
            store(tile, acc, jnp.zeros((1, COLUMN_TILE), jnp.float32))

    @pl.when(jnp.logical_not(small))
    def _():
        @pl.loop(0, tiles)
        def _(tile):
            start = pl.multiple_of(tile * COLUMN_TILE, COLUMN_TILE)
            q = lifted_q[pl.ds(start, COLUMN_TILE), :]

            def visit(b, state):
                acc, peak = state
                at = pl.multiple_of(b * KEY_BLOCK, KEY_BLOCK)
                scores = dot_nt(keys[pl.ds(at, KEY_BLOCK), :], q)
                new = jnp.maximum(peak, jnp.max(scores, axis=0, keepdims=True))
                terms = jnp.exp2(scores - new).astype(jnp.bfloat16)
                acc = acc * jnp.exp2(peak - new) + dot_nn(
                    values_t[:, pl.ds(at, KEY_BLOCK)], terms
                )
                return acc, new

            acc, peak = lax.fori_loop(
                0,
                blocks,
                visit,
                (
                    jnp.zeros((PART_ROWS, COLUMN_TILE), jnp.float32),
                    jnp.full((1, COLUMN_TILE), -3e38, jnp.float32),
                ),
            )
            store(tile, acc, peak)


def attention(queries, gathered, first_lane_block):
    n_tp, tokens, _ = queries.shape
    n_c, n_x, n_z, rows, lanes = gathered.shape
    piece_count = lanes // 128 - first_lane_block
    key_count = n_c * n_x * n_z * rows * piece_count
    columns = n_tp * tokens * 4

    def piece(k):
        return pl.BlockSpec(
            (n_c, n_x, n_z, rows, 128), lambda *_: (0, 0, 0, 0, first_lane_block + k)
        )

    return pl.pallas_call(
        attention_kernel,
        grid=(1,),
        out_shape=jax.ShapeDtypeStruct((n_tp, PART_ROWS, tokens * 4), jnp.bfloat16),
        in_specs=[whole(queries.shape)] + [piece(k) for k in range(piece_count)],
        out_specs=whole((n_tp, PART_ROWS, tokens * 4)),
        scratch_shapes=[
            pltpu.VMEM((key_count, 128), jnp.bfloat16),
            pltpu.VMEM((PART_ROWS, key_count), jnp.bfloat16),
            pltpu.VMEM((columns, 128), jnp.bfloat16),
        ],
        cost_estimate=pl.CostEstimate(
            flops=2 * columns * key_count * 512,
            bytes_accessed=2 * key_count * 128,
            transcendentals=columns * key_count,
        ),
        name="attention",
    )(queries, *([gathered] * piece_count))


def chain_kernel(first_ref, pieces_ref, out_ref):
    def visit(k, state):
        out_ref[k] = state
        return pieces_ref[k, 2:4, :] * state + pieces_ref[k, 0:2, :]

    lax.fori_loop(0, pieces_ref.shape[0], visit, first_ref[...], unroll=8)


def chained(first, pieces):
    count = pieces.shape[0]
    return pl.pallas_call(
        chain_kernel,
        grid=(1,),
        out_shape=jax.ShapeDtypeStruct((count, 2, 128), jnp.float32),
        in_specs=[whole(first.shape), whole(pieces.shape)],
        out_specs=whole((count, 2, 128)),
        name="chained",
    )(first, pieces)


def span_scan(rec_query, inflow_state, rec_values, log_decay_values):
    head_count, row_count, channel_width = rec_query.shape
    span_count = row_count // REC_SPAN

    def to_spans(matrix):
        return jnp.moveaxis(
            matrix.reshape(head_count, span_count, REC_SPAN, matrix.shape[-1]), 1, 0
        )

    lower_mask = jnp.tril(jnp.ones((REC_SPAN, REC_SPAN), jnp.float32))

    def step(carry_pair, inputs):
        carried_state, offset = carry_pair
        query_span, inflow_span, value_segment, decay_span = inputs
        running = jnp.cumsum(decay_span, axis=1)
        segment_final = running[:, -1:, :]
        decayed_query = query_span * jnp.exp(running)
        inflow_dec = inflow_span * jnp.exp(-running)
        within_segment = jnp.einsum("hsk,htk->hst", decayed_query, inflow_dec) * lower_mask
        segment_output = jnp.einsum("rcn,rni->rci", within_segment, value_segment) + jnp.einsum(
            "cwi,cip->cwp", decayed_query, carried_state
        )
        lifted_values = query_span * jnp.exp(offset + running)
        inflow_final = inflow_span * jnp.exp(segment_final - running)
        carried_state = jnp.exp(segment_final)[:, 0, :, None] * carried_state + jnp.einsum(
            "rgc,rgt->rct", inflow_final, value_segment
        )
        return ((carried_state, offset + segment_final), (segment_output, lifted_values))

    initial = (
        jnp.zeros((head_count, channel_width, rec_values.shape[-1]), jnp.float32),
        jnp.zeros((head_count, 1, channel_width), jnp.float32),
    )
    (final_state, offset), (span_outs, lifted_all) = lax.scan(
        step,
        initial,
        (
            to_spans(rec_query),
            to_spans(inflow_state),
            to_spans(rec_values),
            to_spans(log_decay_values),
        ),
    )
    local_output = jnp.moveaxis(span_outs, 0, 1).reshape(
        head_count, row_count, rec_values.shape[-1]
    )
    lifted_values = jnp.moveaxis(lifted_all, 0, 1).reshape(head_count, row_count, channel_width)
    return (final_state, local_output, lifted_values, jnp.exp(offset[:, 0, :]))


def state_before(local_state, reach_decay, initial_recurrent_state):
    members = lax.axis_size(SP)
    rows = local_state.shape[0] * local_state.shape[1]
    share = rows // members
    state_rows = local_state.reshape(members, share, 128)
    decay_rows = jnp.broadcast_to(reach_decay.reshape(members, share, 1), (members, share, 128))
    sent = jnp.concatenate([state_rows, decay_rows], axis=1).astype(jnp.bfloat16)
    arrived = lax.all_to_all(sent, SP, 0, 0, tiled=True).astype(jnp.float32)
    first = lax.dynamic_index_in_dim(
        initial_recurrent_state.reshape(members, share, 128), lax.axis_index(SP), 0, False
    )
    before = chained(first, arrived).astype(jnp.bfloat16)
    back = lax.all_to_all(before, SP, 0, 0, tiled=True)
    return back.reshape(local_state.shape)


def body(
    tokens,
    input_norm_gain,
    paired_query_weight,
    shared_key_weight,
    shared_value_weight,
    recurrent_query_weight,
    forget_gate_weight,
    recurrent_value_weight,
    attention_output_weight,
    recurrent_output_weight,
    attention_head_gain,
    recurrent_head_gain,
    second_map_weight,
    forget_leak_rate,
    extra_log_decay,
    initial_recurrent_state,
):
    attn_heads = paired_query_weight.shape[1] // (2 * QK_DIM)
    rec_heads = recurrent_query_weight.shape[1] // RECURRENT_WIDTH
    out_weights = lax.all_gather(
        jnp.concatenate([attention_output_weight, recurrent_output_weight], axis=1),
        SP,
        axis=0,
        tiled=True,
    )
    own_normed = rms_scale(tokens.astype(jnp.float32), input_norm_gain).astype(jnp.bfloat16)
    own_rows = own_normed.shape[0]
    key_value = project(
        own_normed, jnp.concatenate([shared_key_weight, shared_value_weight], axis=1)
    )
    piece_rows = paired_query_weight.shape[0]
    payload = jnp.concatenate(
        [paired_query_weight, recurrent_query_weight, forget_gate_weight, recurrent_value_weight]
        + [key_value[k * piece_rows : (k + 1) * piece_rows] for k in range(own_rows // piece_rows)],
        axis=1,
    )
    along_z = sent_to_all(payload, "z")
    gathered = sent_to_all(sent_to_all(along_z, "x"), "c")
    normed = lax.all_gather(own_normed, "tp", axis=0, tiled=True)
    row_count = normed.shape[0]
    narrow = paired_query_weight.shape[1]
    recur = 3 * rec_heads * RECURRENT_WIDTH
    queries, recur_raw = projections(gathered, normed, narrow, recur)
    all_queries = lax.all_gather(queries, "tp", axis=0)
    parts = attention(all_queries, gathered, (narrow + recur) // 128)

    wide = rec_heads * RECURRENT_WIDTH
    rec_query = jax.nn.silu(recur_raw[:, :wide].astype(jnp.float32))
    gate_raw = recur_raw[:, wide : 2 * wide].astype(jnp.float32)
    rec_values = recur_raw[:, 2 * wide :].astype(jnp.float32)
    inflow_state = forget_leak_rate * (1.0 - jax.nn.sigmoid(gate_raw))
    log_decay_values = jnp.log(1.0 - inflow_state) + extra_log_decay

    def heads_first(matrix):
        return matrix.reshape(row_count, rec_heads, RECURRENT_WIDTH).transpose(1, 0, 2)

    local_state, local_output, lifted_values, reach_decay = span_scan(
        heads_first(rec_query),
        heads_first(inflow_state),
        heads_first(rec_values),
        heads_first(log_decay_values),
    )
    incoming_state = state_before(local_state, reach_decay, initial_recurrent_state)
    recurrent_output = local_output + jnp.einsum(
        "cwi,cip->cwp", lifted_values, incoming_state.astype(jnp.float32)
    )
    rec_hidden = (
        rms_scale(recurrent_output, recurrent_head_gain)
        .transpose(1, 0, 2)
        .reshape(row_count, rec_heads * RECURRENT_WIDTH)
        .astype(jnp.bfloat16)
    )

    arrived = lax.all_to_all(parts, "tp", 0, 0, tiled=True).astype(jnp.float32)


    def joined(first_row):
        row = HEAD_DIM + first_row
        return arrived[:, row : row + 1] + arrived[:, row + 1 : row + 2] + arrived[:, row + 2 : row + 3]

    shift = joined(3)
    factor = jnp.exp2(shift - jnp.max(shift, axis=0, keepdims=True))
    weighted = jnp.sum(arrived[:, :HEAD_DIM] * factor, axis=0)
    totals = jnp.sum(joined(0) * factor, axis=0)
    ratio = (weighted / totals).reshape(HEAD_DIM, attn_heads, 2, row_count)
    blended = ratio[:, :, 0] - second_map_weight[None, :, None] * ratio[:, :, 1]
    attn_hidden = (
        blended
        * lax.rsqrt(jnp.mean(blended * blended, axis=0, keepdims=True) + epsilon)
        * attention_head_gain[:, None, None]
    ).astype(jnp.bfloat16)
    attn_hidden = attn_hidden.transpose(1, 0, 2).reshape(attn_heads * HEAD_DIM, row_count)
    attn_wide = attn_heads * HEAD_DIM
    partial = (
        jnp.einsum(
            "kt,dk->td", attn_hidden, out_weights[:, :attn_wide], preferred_element_type=jnp.float32
        )
        + jnp.einsum(
            "tk,dk->td", rec_hidden, out_weights[:, attn_wide:], preferred_element_type=jnp.float32
        )
    ).astype(jnp.bfloat16)
    size = lax.axis_size("tp")
    blocks = partial.reshape(size, row_count // size, partial.shape[1])
    landed = lax.all_to_all(blocks, "tp", 0, 0, tiled=True)
    return landed.astype(jnp.float32).sum(axis=0).astype(jnp.bfloat16)


def solution(mesh):
    torus = Mesh(mesh.devices.reshape(16, 4, 2, mesh.shape["tp"]), SP_TP)
    placed = (
        P(SP_TP, None),
        P(),
        P(SP, "tp"),
        P(),
        P(),
        P(SP, "tp"),
        P(SP, "tp"),
        P(SP, "tp"),
        P(SP, "tp"),
        P(SP, "tp"),
        P(),
        P(),
        P("tp"),
        P("tp"),
        P(SP, "tp"),
        P("tp", None, None),
    )
    return jax.shard_map(
        body, mesh=torus, in_specs=placed, out_specs=P(SP_TP, None), check_vma=False
    )
```

```python
import functools
import math

import jax
import jax.numpy as jnp
from jax import lax
from jax.experimental import pallas as pl
from jax.experimental.pallas import tpu as pltpu
from jax.sharding import Mesh
from jax.sharding import PartitionSpec as P

QK_DIM = 32
HEAD_DIM = 64
RECURRENT_WIDTH = 128
REC_SPAN = 64
SP = ("z", "x", "c")
SP_TP = ("z", "x", "c", "tp")
KEY_BLOCK = 256
COLUMN_TILE = 256
PART_ROWS = 80

epsilon = 1e-06


def sent_to_all(x, axis):
    size = lax.axis_size(axis)
    return lax.all_to_all(jnp.broadcast_to(x[None], (size, *x.shape)), axis, 0, 0, tiled=True)


def rms_scale(matrix, gain):
    return matrix * lax.rsqrt(jnp.mean(matrix * matrix, axis=-1, keepdims=True) + epsilon) * gain


def project(normed, weight):
    return jnp.dot(normed, weight, preferred_element_type=jnp.float32).astype(jnp.bfloat16)


def whole(shape):
    return pl.BlockSpec(shape, lambda *_: (0,) * len(shape))


def dot_nt(a, b):
    return lax.dot_general(a, b, (((1,), (1,)), ((), ())), preferred_element_type=jnp.float32)


def dot_nn(a, b):
    return jnp.dot(a, b, preferred_element_type=jnp.float32)


def ordered_rows(core_ref, own_ref, other_ref, lanes, ordered):
    n_x, n_z, rows = own_ref.shape[:3]
    core = core_ref[0]
    for z in range(n_z):
        for x in range(n_x):
            start = (z * n_x + x) * 2 * rows
            mine = pl.multiple_of(start + core * rows, rows)
            others = pl.multiple_of(start + (1 - core) * rows, rows)
            ordered[pl.ds(mine, rows), :] = own_ref[x, z, :, lanes]
            ordered[pl.ds(others, rows), :] = other_ref[x, z, :, lanes]


def projection_kernel(core_ref, own_ref, other_ref, normed_ref, out_ref, ordered):
    wide = out_ref.shape[1]
    ordered_rows(core_ref, own_ref, other_ref, slice(0, wide), ordered)
    normed = normed_ref[...]
    step = min(wide, 256)
    for k in range(wide // step):
        span = slice(k * step, (k + 1) * step)
        out_ref[:, span] = dot_nn(normed, ordered[:, span]).astype(jnp.bfloat16)


def in_smem():
    return pl.BlockSpec(memory_space=pltpu.SMEM)


def projections(core, own, other, normed, wide, name):
    tokens, width = normed.shape
    piece = (*own.shape[:3], wide)
    return pl.pallas_call(
        projection_kernel,
        grid=(1,),
        out_shape=jax.ShapeDtypeStruct((tokens, wide), jnp.bfloat16),
        in_specs=[in_smem(), whole(piece), whole(piece), whole(normed.shape)],
        out_specs=whole((tokens, wide)),
        scratch_shapes=[pltpu.VMEM((width, wide), jnp.bfloat16)],
        cost_estimate=pl.CostEstimate(
            flops=2 * tokens * width * wide, bytes_accessed=2 * width * wide, transcendentals=0
        ),
        name=name,
    )(core, own, other, normed)


def one_hot(rows, cols, row_offset, col_offset, count):
    r = lax.broadcasted_iota(jnp.int32, (rows, cols), 0) - row_offset
    c = lax.broadcasted_iota(jnp.int32, (rows, cols), 1) - col_offset
    hit = (r == c) & (r >= 0) & (r < count)
    return jnp.where(hit, 1.0, 0.0).astype(jnp.bfloat16)


def attention_kernel(query_ref, *refs):
    key_value_refs, (out_ref, keys, values_t, lifted_q) = refs[:-4], refs[-4:]
    n_tp, tokens, _ = query_ref.shape
    n_x, n_z, rows, _ = key_value_refs[0].shape
    piece_rows = n_z * rows
    both = 2 * QK_DIM
    twice = one_hot(128, 128, 0, 0, both) + one_hot(128, 128, 0, both, both)
    pick_values = one_hot(PART_ROWS, 128, 0, both, HEAD_DIM)
    ones_row = jnp.where(
        lax.broadcasted_iota(jnp.int32, (PART_ROWS, piece_rows), 0) == HEAD_DIM, 1.0, 0.0
    )
    key_peak = jnp.zeros((8, 128), jnp.float32)
    index = 0
    for ref in key_value_refs:
        for x in range(n_x):
            piece = ref[x].reshape(piece_rows, 128)
            at = index * piece_rows
            doubled = dot_nn(piece, twice)
            keys[at : at + piece_rows, :] = doubled.astype(jnp.bfloat16)
            size = jnp.abs(doubled).reshape(piece_rows // 8, 8, 128)
            key_peak = jnp.maximum(key_peak, jnp.max(size, axis=0))
            values_t[:, at : at + piece_rows] = (
                dot_nt(pick_values, piece) + ones_row
            ).astype(jnp.bfloat16)
            index += 1
    key_count = index * piece_rows
    scale = math.log2(math.e) / math.sqrt(QK_DIM)
    lane = lax.broadcasted_iota(jnp.int32, (tokens, 128), 1) % both
    for tp in range(n_tp):
        scaled = query_ref[tp].astype(jnp.float32) * scale
        high = scaled.astype(jnp.bfloat16)
        low = (scaled - high.astype(jnp.float32)).astype(jnp.bfloat16)
        for head in range(2):
            spread = dot_nn(high, one_hot(128, 128, head * both, 0, both)) + dot_nn(
                low, one_hot(128, 128, head * both, both, both)
            )
            for part in range(2):
                own = (lane >= part * QK_DIM) & (lane < (part + 1) * QK_DIM)
                at = ((tp * 2 + part) * 2 + head) * tokens
                lifted_q[at : at + tokens, :] = jnp.where(own, spread, 0.0).astype(jnp.bfloat16)
    peak_row = jnp.max(key_peak, axis=0, keepdims=True) * 1.02
    bound = dot_nt(
        jnp.broadcast_to(peak_row, (8, 128)).astype(jnp.bfloat16), jnp.abs(lifted_q[...])
    )
    small = jnp.max(bound) < 100.0
    blocks = key_count // KEY_BLOCK
    tiles = lifted_q.shape[0] // COLUMN_TILE
    per_group = tiles // n_tp

    def store(tile, acc, shift):
        group, place = tile // per_group, tile % per_group
        at = pl.multiple_of(place * COLUMN_TILE, COLUMN_TILE)
        row = lax.broadcasted_iota(jnp.int32, (PART_ROWS - HEAD_DIM, COLUMN_TILE), 0)
        tail = jnp.zeros(row.shape, jnp.float32)
        slot = 0
        for rest in (acc[HEAD_DIM : HEAD_DIM + 1, :], shift):
            for _ in range(3):
                high = rest.astype(jnp.bfloat16).astype(jnp.float32)
                tail = jnp.where(row == slot, high, tail)
                rest = rest - high
                slot += 1
        out_ref[group, :HEAD_DIM, pl.ds(at, COLUMN_TILE)] = acc[:HEAD_DIM, :].astype(jnp.bfloat16)
        out_ref[group, HEAD_DIM:, pl.ds(at, COLUMN_TILE)] = tail.astype(jnp.bfloat16)

    @pl.when(small)
    def _():
        @pl.loop(0, tiles)
        def _(tile):
            start = pl.multiple_of(tile * COLUMN_TILE, COLUMN_TILE)
            q = lifted_q[pl.ds(start, COLUMN_TILE), :]
            acc = jnp.zeros((PART_ROWS, COLUMN_TILE), jnp.float32)
            for b in range(blocks):
                span = slice(b * KEY_BLOCK, (b + 1) * KEY_BLOCK)
                scores = dot_nt(keys[span, :], q)
                acc = acc + dot_nn(values_t[:, span], jnp.exp2(scores).astype(jnp.bfloat16))
            store(tile, acc, jnp.zeros((1, COLUMN_TILE), jnp.float32))

    @pl.when(jnp.logical_not(small))
    def _():
        @pl.loop(0, tiles)
        def _(tile):
            start = pl.multiple_of(tile * COLUMN_TILE, COLUMN_TILE)
            q = lifted_q[pl.ds(start, COLUMN_TILE), :]

            def visit(b, state):
                acc, peak = state
                at = pl.multiple_of(b * KEY_BLOCK, KEY_BLOCK)
                scores = dot_nt(keys[pl.ds(at, KEY_BLOCK), :], q)
                new = jnp.maximum(peak, jnp.max(scores, axis=0, keepdims=True))
                terms = jnp.exp2(scores - new).astype(jnp.bfloat16)
                acc = acc * jnp.exp2(peak - new) + dot_nn(
                    values_t[:, pl.ds(at, KEY_BLOCK)], terms
                )
                return acc, new

            acc, peak = lax.fori_loop(
                0,
                blocks,
                visit,
                (
                    jnp.zeros((PART_ROWS, COLUMN_TILE), jnp.float32),
                    jnp.full((1, COLUMN_TILE), -3e38, jnp.float32),
                ),
            )
            store(tile, acc, peak)


def attention(queries, sources, first_lane_block, piece_count):
    n_tp, tokens, _ = queries.shape
    n_x, n_z, rows, _ = sources[0].shape
    key_count = n_x * n_z * rows * piece_count * len(sources)
    columns = n_tp * tokens * 4

    def piece(k):
        return pl.BlockSpec((n_x, n_z, rows, 128), lambda *_: (0, 0, 0, first_lane_block + k))

    return pl.pallas_call(
        attention_kernel,
        grid=(1,),
        out_shape=jax.ShapeDtypeStruct((n_tp, PART_ROWS, tokens * 4), jnp.bfloat16),
        in_specs=[whole(queries.shape)] + [piece(k) for k in range(piece_count)] * len(sources),
        out_specs=whole((n_tp, PART_ROWS, tokens * 4)),
        scratch_shapes=[
            pltpu.VMEM((key_count, 128), jnp.bfloat16),
            pltpu.VMEM((PART_ROWS, key_count), jnp.bfloat16),
            pltpu.VMEM((columns, 128), jnp.bfloat16),
        ],
        cost_estimate=pl.CostEstimate(
            flops=2 * columns * key_count * 512,
            bytes_accessed=2 * key_count * 128,
            transcendentals=columns * key_count,
        ),
        name="attention",
    )(queries, *[source for source in sources for _ in range(piece_count)])


def in_three(matrix):
    high = matrix.astype(jnp.bfloat16)
    rest = matrix - high.astype(jnp.float32)
    middle = rest.astype(jnp.bfloat16)
    return high, middle, (rest - middle.astype(jnp.float32)).astype(jnp.bfloat16)


def recurrence_kernel(raw_ref, leak_ref, extra_ref, local_ref, lifted_ref, state_ref, decay_ref):
    rows, wide = extra_ref.shape
    heads = wide // RECURRENT_WIDTH
    raw_query = raw_ref[:, :wide].astype(jnp.float32)
    raw_gate = raw_ref[:, wide : 2 * wide].astype(jnp.float32)
    query = raw_query * jax.nn.sigmoid(raw_query)
    inflow = leak_ref[...] * (1.0 - jax.nn.sigmoid(raw_gate))
    log_decay = jnp.log(1.0 - inflow) + extra_ref[...]
    lower = lax.broadcasted_iota(jnp.int32, (REC_SPAN, REC_SPAN), 0) >= lax.broadcasted_iota(
        jnp.int32, (REC_SPAN, REC_SPAN), 1
    )
    triangle = jnp.where(lower, 1.0, 0.0).astype(jnp.bfloat16)
    offset = jnp.zeros((1, wide), jnp.float32)
    states = [jnp.zeros((RECURRENT_WIDTH, RECURRENT_WIDTH), jnp.float32)] * heads
    for span in range(rows // REC_SPAN):
        part = slice(span * REC_SPAN, (span + 1) * REC_SPAN)
        running = sum(dot_nn(triangle, term) for term in in_three(log_decay[part]))
        final = running[REC_SPAN - 1 :, :]
        decayed = query[part] * jnp.exp(running)
        lifted = query[part] * jnp.exp(offset + running)
        opened = (inflow[part] * jnp.exp(-running)).astype(jnp.bfloat16)
        closing = (inflow[part] * jnp.exp(final - running)).astype(jnp.bfloat16)
        kept = jnp.exp(final)
        offset = offset + final
        for head in range(heads):
            lanes = slice(head * RECURRENT_WIDTH, (head + 1) * RECURRENT_WIDTH)
            values = raw_ref[part, 2 * wide + lanes.start : 2 * wide + lanes.stop]
            mine = decayed[:, lanes].astype(jnp.bfloat16)
            within = jnp.where(lower, dot_nt(mine, opened[:, lanes]), 0.0)
            local = dot_nn(within.astype(jnp.bfloat16), values)
            if span > 0:
                local = local + dot_nt(mine, states[head].astype(jnp.bfloat16))
            local_ref[head, part, :] = local
            lifted_ref[head, part, :] = lifted[:, lanes].astype(jnp.bfloat16)
            states[head] = kept[:, lanes] * states[head] + lax.dot_general(
                values, closing[:, lanes], (((0,), (0,)), ((), ())),
                preferred_element_type=jnp.float32,
            )
    for head in range(heads):
        state_ref[head] = states[head]
        lanes = slice(head * RECURRENT_WIDTH, (head + 1) * RECURRENT_WIDTH)
        decay_ref[head] = jnp.exp(offset[:, lanes])


def local_recurrence(raw, leak, extra):
    rows, wide = extra.shape
    heads = wide // RECURRENT_WIDTH
    by_head = (heads, rows, RECURRENT_WIDTH)
    square = (heads, RECURRENT_WIDTH, RECURRENT_WIDTH)
    line = (heads, 1, RECURRENT_WIDTH)
    return pl.pallas_call(
        recurrence_kernel,
        grid=(1,),
        out_shape=(
            jax.ShapeDtypeStruct(by_head, jnp.float32),
            jax.ShapeDtypeStruct(by_head, jnp.bfloat16),
            jax.ShapeDtypeStruct(square, jnp.float32),
            jax.ShapeDtypeStruct(line, jnp.float32),
        ),
        in_specs=[whole(raw.shape), whole(leak.shape), whole(extra.shape)],
        out_specs=(whole(by_head), whole(by_head), whole(square), whole(line)),
        cost_estimate=pl.CostEstimate(
            flops=2 * rows * wide * 1024, bytes_accessed=8 * rows * wide, transcendentals=0
        ),
        name="recurrence",
    )(raw, leak, extra)


def chain_kernel(first_ref, pieces_ref, out_ref):
    def visit(k, state):
        out_ref[k] = state.astype(jnp.bfloat16)
        piece = pieces_ref[k].astype(jnp.float32)
        return piece[2:3, :] * state + piece[0:2, :]

    lax.fori_loop(0, pieces_ref.shape[0], visit, first_ref[...], unroll=8)


def chained(first, pieces):
    count = pieces.shape[0]
    return pl.pallas_call(
        chain_kernel,
        grid=(1,),
        out_shape=jax.ShapeDtypeStruct((count, 2, 128), jnp.bfloat16),
        in_specs=[whole(first.shape), whole(pieces.shape)],
        out_specs=whole((count, 2, 128)),
        name="chained",
    )(first, pieces)


def state_before(local_state, reach_decay, initial_recurrent_state):
    members = lax.axis_size(SP)
    heads, width, _ = local_state.shape
    share = heads * width // members
    state_rows = local_state.reshape(members, share, 128)
    decay_rows = jnp.broadcast_to(
        reach_decay[:, None], (heads, members // heads, 1, 128)
    ).reshape(members, 1, 128)
    sent = jnp.concatenate(
        [state_rows, decay_rows, jnp.zeros_like(decay_rows)], axis=1
    ).astype(jnp.bfloat16)
    arrived = lax.all_to_all(sent, SP, 0, 0, tiled=True)
    first = lax.dynamic_index_in_dim(
        initial_recurrent_state.transpose(0, 2, 1).reshape(members, share, 128),
        lax.axis_index(SP),
        0,
        False,
    )
    back = lax.all_to_all(chained(first, arrived), SP, 0, 0, tiled=True)
    return back.reshape(local_state.shape)


def output_kernel(
    core_ref,
    second_ref,
    parts_ref,
    attn_gain_ref,
    local_ref,
    lifted_ref,
    state_ref,
    rec_gain_ref,
    own_ref,
    other_ref,
    out_ref,
    ordered,
):
    n_lanes = ordered.shape[1]
    first = own_ref.shape[3] - n_lanes
    ordered_rows(core_ref, own_ref, other_ref, slice(first, first + n_lanes), ordered)
    members = parts_ref.shape[0]
    tokens = local_ref.shape[1]
    columns = parts_ref.shape[2]
    half = columns // 2

    def joined(k, row):
        lines = parts_ref[k, HEAD_DIM:, :].astype(jnp.float32)
        return lines[row : row + 1] + lines[row + 1 : row + 2] + lines[row + 2 : row + 3]

    shifts = [joined(k, 3) for k in range(members)]
    top = functools.reduce(jnp.maximum, shifts)
    weighted = jnp.zeros((HEAD_DIM, columns), jnp.float32)
    totals = jnp.zeros((1, columns), jnp.float32)
    for k in range(members):
        factor = jnp.exp2(shifts[k] - top)
        weighted = weighted + parts_ref[k, :HEAD_DIM, :].astype(jnp.float32) * factor
        totals = totals + joined(k, 0) * factor
    ratio = weighted / totals
    head_of = lax.broadcasted_iota(jnp.int32, (1, half), 1) >= tokens
    second = jnp.where(head_of, second_ref[1], second_ref[0])
    blended = ratio[:, :half] - second * ratio[:, half:]
    scale = lax.rsqrt(jnp.mean(blended * blended, axis=0, keepdims=True) + epsilon)
    hidden_t = blended * scale * attn_gain_ref[...]
    turned = jnp.concatenate([hidden_t, hidden_t], axis=0).T
    lane = lax.broadcasted_iota(jnp.int32, (tokens, 2 * HEAD_DIM), 1)
    hidden = [jnp.where(lane < HEAD_DIM, turned[:tokens], turned[tokens:]).astype(jnp.bfloat16)]
    for head in range(local_ref.shape[0]):
        rec = local_ref[head] + dot_nt(lifted_ref[head], state_ref[head])
        scale = lax.rsqrt(jnp.mean(rec * rec, axis=1, keepdims=True) + epsilon)
        hidden.append((rec * scale * rec_gain_ref[...]).astype(jnp.bfloat16))
    hidden = jnp.concatenate(hidden, axis=1)
    step = 512
    for k in range(out_ref.shape[1] // step):
        span = slice(k * step, (k + 1) * step)
        out_ref[:, span] = dot_nt(hidden, ordered[span, :]).astype(jnp.bfloat16)


def output_partial(core, second, parts, attn_gain, local, lifted, state, rec_gain, own, other):
    heads, tokens, width = local.shape
    n_x, n_z, rows, lanes = own.shape
    model = n_x * n_z * rows * 2
    mixed = parts.shape[2] // (2 * tokens) * HEAD_DIM + heads * width
    arrays = (parts, attn_gain, local, lifted, state, rec_gain, own, other)
    return pl.pallas_call(
        output_kernel,
        grid=(1,),
        out_shape=jax.ShapeDtypeStruct((tokens, model), jnp.bfloat16),
        in_specs=[in_smem(), in_smem()] + [whole(a.shape) for a in arrays],
        out_specs=whole((tokens, model)),
        scratch_shapes=[pltpu.VMEM((model, mixed), jnp.bfloat16)],
        cost_estimate=pl.CostEstimate(
            flops=2 * tokens * model * mixed, bytes_accessed=2 * model * mixed, transcendentals=0
        ),
        name="output_partial",
    )(core, second, *arrays)


def body(
    tokens,
    input_norm_gain,
    paired_query_weight,
    shared_key_weight,
    shared_value_weight,
    recurrent_query_weight,
    forget_gate_weight,
    recurrent_value_weight,
    attention_output_weight,
    recurrent_output_weight,
    attention_head_gain,
    recurrent_head_gain,
    second_map_weight,
    forget_leak_rate,
    extra_log_decay,
    initial_recurrent_state,
):
    core = lax.axis_index("c").astype(jnp.int32).reshape(1)
    own_normed = rms_scale(tokens.astype(jnp.float32), input_norm_gain).astype(jnp.bfloat16)
    own_rows = own_normed.shape[0]
    first_payload = jnp.concatenate(
        [recurrent_query_weight, forget_gate_weight, recurrent_value_weight], axis=1
    )
    key_value = project(
        own_normed, jnp.concatenate([shared_key_weight, shared_value_weight], axis=1)
    )
    rows = paired_query_weight.shape[0]
    narrow = paired_query_weight.shape[1]
    kv_pieces = own_rows // rows
    second_payload = jnp.concatenate(
        [paired_query_weight]
        + [key_value[k * rows : (k + 1) * rows] for k in range(kv_pieces)]
        + [attention_output_weight, recurrent_output_weight],
        axis=1,
    )
    swap = [(0, 1), (1, 0)]
    first_z = sent_to_all(first_payload, "z")
    normed = lax.all_gather(own_normed, "tp", axis=0, tiled=True)
    second_payload, first_z, normed = lax.optimization_barrier((second_payload, first_z, normed))
    first_own = sent_to_all(first_z, "x")
    first_other = lax.ppermute(first_own, "c", swap)
    recur = first_payload.shape[1]
    recur_raw = projections(core, first_own, first_other, normed, recur, "project_recurrence")
    local_output, lifted, local_state, reach_decay = local_recurrence(
        recur_raw, forget_leak_rate[None, :], extra_log_decay
    )
    second_z = sent_to_all(second_payload, "z")
    second_own = sent_to_all(second_z, "x")
    second_other = lax.ppermute(second_own, "c", swap)
    incoming_state = state_before(local_state, reach_decay, initial_recurrent_state)
    queries = projections(core, second_own, second_other, normed, narrow, "project_queries")
    all_queries = sent_to_all(queries, "tp")
    parts = attention(all_queries, (second_own, second_other), narrow // 128, kv_pieces)
    arrived = lax.all_to_all(parts, "tp", 0, 0, tiled=True)
    partial = output_partial(
        core,
        second_map_weight,
        arrived,
        attention_head_gain[:, None],
        local_output,
        lifted,
        incoming_state,
        recurrent_head_gain[None, :],
        second_own,
        second_other,
    )
    size = lax.axis_size("tp")
    blocks = partial.reshape(size, own_rows, partial.shape[1])
    landed = lax.all_to_all(blocks, "tp", 0, 0, tiled=True)
    return landed.astype(jnp.float32).sum(axis=0).astype(jnp.bfloat16)


def solution(mesh):
    torus = Mesh(mesh.devices.reshape(16, 4, 2, mesh.shape["tp"]), SP_TP)
    placed = (
        P(SP_TP, None),
        P(),
        P(SP, "tp"),
        P(),
        P(),
        P(SP, "tp"),
        P(SP, "tp"),
        P(SP, "tp"),
        P(SP, "tp"),
        P(SP, "tp"),
        P(),
        P(),
        P("tp"),
        P("tp"),
        P(SP, "tp"),
        P("tp", None, None),
    )
    return jax.shard_map(
        body, mesh=torus, in_specs=placed, out_specs=P(SP_TP, None), check_vma=False
    )
```

```python
import functools
import math

import jax
import jax.numpy as jnp
from jax import lax
from jax.experimental import pallas as pl
from jax.experimental.pallas import tpu as pltpu
from jax.sharding import Mesh
from jax.sharding import PartitionSpec as P


QK_DIM = 32
HEAD_DIM = 64
RECURRENT_WIDTH = 128
REC_SPAN = 64
SP = ("z", "x", "c")
SP_TP = ("z", "x", "c", "tp")
KEY_BLOCK = 512
COLUMN_TILE = 256
PART_ROWS = 80

epsilon = 1e-06


def sent_to_all(x, axis):
    size = lax.axis_size(axis)
    return lax.all_to_all(jnp.broadcast_to(x[None], (size, *x.shape)), axis, 0, 0, tiled=True)


def from_others(x, axis):
    size = lax.axis_size(axis)
    pieces = [x] + [
        lax.ppermute(x, axis, [((k + ahead) % size, k) for k in range(size)])
        for ahead in range(1, size)
    ]
    return jnp.stack(pieces)


def rms_scale(matrix, gain):
    return matrix * lax.rsqrt(jnp.mean(matrix * matrix, axis=-1, keepdims=True) + epsilon) * gain


def project(normed, weight):
    return jnp.dot(normed, weight, preferred_element_type=jnp.float32).astype(jnp.bfloat16)


def whole(shape):
    return pl.BlockSpec(shape, lambda *_: (0,) * len(shape))


def dot_nt(a, b):
    return lax.dot_general(a, b, (((1,), (1,)), ((), ())), preferred_element_type=jnp.float32)


def dot_nn(a, b):
    return jnp.dot(a, b, preferred_element_type=jnp.float32)


def ordered_rows(place_ref, own_ref, other_ref, lanes, ordered):
    n_x, n_z, rows = own_ref.shape[:3]
    core = place_ref[0]
    for x in range(n_x):
        owner = lax.rem(place_ref[1] + x, n_x)
        for z in range(n_z):
            start = (z * n_x + owner) * 2 * rows
            mine = pl.multiple_of(start + core * rows, rows)
            others = pl.multiple_of(start + (1 - core) * rows, rows)
            ordered[pl.ds(mine, rows), :] = own_ref[x, z, :, lanes]
            ordered[pl.ds(others, rows), :] = other_ref[x, z, :, lanes]


def projection_kernel(place_ref, own_ref, other_ref, normed_ref, out_ref, ordered):
    wide = out_ref.shape[1]
    ordered_rows(place_ref, own_ref, other_ref, slice(0, wide), ordered)
    normed = normed_ref[...]
    step = min(wide, 256)
    for k in range(wide // step):
        span = slice(k * step, (k + 1) * step)
        out_ref[:, span] = dot_nn(normed, ordered[:, span]).astype(jnp.bfloat16)


def in_smem():
    return pl.BlockSpec(memory_space=pltpu.SMEM)


def projections(place, own, other, normed, wide):
    tokens, width = normed.shape
    piece = (*own.shape[:3], wide)
    return pl.pallas_call(
        projection_kernel,
        grid=(1,),
        out_shape=jax.ShapeDtypeStruct((tokens, wide), jnp.bfloat16),
        in_specs=[in_smem(), whole(piece), whole(piece), whole(normed.shape)],
        out_specs=whole((tokens, wide)),
        scratch_shapes=[pltpu.VMEM((width, wide), jnp.bfloat16)],
        cost_estimate=pl.CostEstimate(
            flops=2 * tokens * width * wide, bytes_accessed=2 * width * wide, transcendentals=0
        ),
    )(place, own, other, normed)


def one_hot(rows, cols, row_offset, col_offset, count):
    r = lax.broadcasted_iota(jnp.int32, (rows, cols), 0) - row_offset
    c = lax.broadcasted_iota(jnp.int32, (rows, cols), 1) - col_offset
    hit = (r == c) & (r >= 0) & (r < count)
    return jnp.where(hit, 1.0, 0.0).astype(jnp.bfloat16)


def attention_kernel(query_ref, *refs):
    key_value_refs, (out_ref, keys, values_t, lifted_q) = refs[:-4], refs[-4:]
    n_tp, tokens, _ = query_ref.shape
    n_x, n_z, rows, _ = key_value_refs[0].shape
    piece_rows = n_z * rows
    both = 2 * QK_DIM
    twice = one_hot(128, 128, 0, 0, both) + one_hot(128, 128, 0, both, both)
    pick_values = one_hot(PART_ROWS, 128, 0, both, HEAD_DIM)
    ones_row = jnp.where(
        lax.broadcasted_iota(jnp.int32, (PART_ROWS, piece_rows), 0) == HEAD_DIM, 1.0, 0.0
    )
    key_peak = jnp.zeros((8, 128), jnp.float32)
    index = 0
    for ref in key_value_refs:
        for x in range(n_x):
            piece = ref[x].reshape(piece_rows, 128)
            at = index * piece_rows
            doubled = dot_nn(piece, twice)
            keys[at : at + piece_rows, :] = doubled.astype(jnp.bfloat16)
            size = jnp.abs(doubled).reshape(piece_rows // 8, 8, 128)
            key_peak = jnp.maximum(key_peak, jnp.max(size, axis=0))
            values_t[:, at : at + piece_rows] = (
                dot_nt(pick_values, piece) + ones_row
            ).astype(jnp.bfloat16)
            index += 1
    key_count = index * piece_rows
    scale = math.log2(math.e) / math.sqrt(QK_DIM)
    lane = lax.broadcasted_iota(jnp.int32, (tokens, 128), 1) % both
    for tp in range(n_tp):
        scaled = query_ref[tp].astype(jnp.float32) * scale
        high = scaled.astype(jnp.bfloat16)
        low = (scaled - high.astype(jnp.float32)).astype(jnp.bfloat16)
        for head in range(2):
            spread = dot_nn(high, one_hot(128, 128, head * both, 0, both)) + dot_nn(
                low, one_hot(128, 128, head * both, both, both)
            )
            for part in range(2):
                own = (lane >= part * QK_DIM) & (lane < (part + 1) * QK_DIM)
                at = ((tp * 2 + part) * 2 + head) * tokens
                lifted_q[at : at + tokens, :] = jnp.where(own, spread, 0.0).astype(jnp.bfloat16)
    peak_row = jnp.max(key_peak, axis=0, keepdims=True) * 1.02
    bound = dot_nt(
        jnp.broadcast_to(peak_row, (8, 128)).astype(jnp.bfloat16), jnp.abs(lifted_q[...])
    )
    small = jnp.max(bound) < 100.0
    blocks = key_count // KEY_BLOCK
    tiles = lifted_q.shape[0] // COLUMN_TILE
    per_group = tiles // n_tp

    def store(tile, acc, shift):
        group, place = tile // per_group, tile % per_group
        at = pl.multiple_of(place * COLUMN_TILE, COLUMN_TILE)
        row = lax.broadcasted_iota(jnp.int32, (PART_ROWS - HEAD_DIM, COLUMN_TILE), 0)
        tail = jnp.zeros(row.shape, jnp.float32)
        slot = 0
        for rest in (acc[HEAD_DIM : HEAD_DIM + 1, :], shift):
            for _ in range(3):
                high = rest.astype(jnp.bfloat16).astype(jnp.float32)
                tail = jnp.where(row == slot, high, tail)
                rest = rest - high
                slot += 1
        out_ref[group, :HEAD_DIM, pl.ds(at, COLUMN_TILE)] = acc[:HEAD_DIM, :].astype(jnp.bfloat16)
        out_ref[group, HEAD_DIM:, pl.ds(at, COLUMN_TILE)] = tail.astype(jnp.bfloat16)

    @pl.when(small)
    def _():
        @pl.loop(0, n_tp)
        def _(group):
            first = group * per_group

            def queries_of(place):
                start = pl.multiple_of((first + place) * COLUMN_TILE, COLUMN_TILE)
                return lifted_q[pl.ds(start, COLUMN_TILE), :]

            def scores_of(place, b):
                return dot_nt(keys[b * KEY_BLOCK : (b + 1) * KEY_BLOCK, :], queries_of(place))

            visits = [(place, b) for place in range(per_group) for b in range(blocks)]
            scores = scores_of(*visits[0])
            acc = None
            for turn, (place, b) in enumerate(visits):
                ahead = scores_of(*visits[turn + 1]) if turn + 1 < len(visits) else None
                terms = jnp.exp2(scores).astype(jnp.bfloat16)
                product = dot_nn(values_t[:, b * KEY_BLOCK : (b + 1) * KEY_BLOCK], terms)
                acc = product if b == 0 else acc + product
                if b == blocks - 1:
                    store(first + place, acc, jnp.zeros((1, COLUMN_TILE), jnp.float32))
                scores = ahead

    @pl.when(jnp.logical_not(small))
    def _():
        @pl.loop(0, tiles)
        def _(tile):
            start = pl.multiple_of(tile * COLUMN_TILE, COLUMN_TILE)
            q = lifted_q[pl.ds(start, COLUMN_TILE), :]

            def visit(b, state):
                acc, peak = state
                at = pl.multiple_of(b * KEY_BLOCK, KEY_BLOCK)
                scores = dot_nt(keys[pl.ds(at, KEY_BLOCK), :], q)
                new = jnp.maximum(peak, jnp.max(scores, axis=0, keepdims=True))
                terms = jnp.exp2(scores - new).astype(jnp.bfloat16)
                acc = acc * jnp.exp2(peak - new) + dot_nn(
                    values_t[:, pl.ds(at, KEY_BLOCK)], terms
                )
                return acc, new

            acc, peak = lax.fori_loop(
                0,
                blocks,
                visit,
                (
                    jnp.zeros((PART_ROWS, COLUMN_TILE), jnp.float32),
                    jnp.full((1, COLUMN_TILE), -3e38, jnp.float32),
                ),
            )
            store(tile, acc, peak)


def attention(queries, sources, first_lane_block, piece_count):
    n_tp, tokens, _ = queries.shape
    n_x, n_z, rows, _ = sources[0].shape
    key_count = n_x * n_z * rows * piece_count * len(sources)
    columns = n_tp * tokens * 4

    def piece(k):
        return pl.BlockSpec((n_x, n_z, rows, 128), lambda *_: (0, 0, 0, first_lane_block + k))

    return pl.pallas_call(
        attention_kernel,
        grid=(1,),
        out_shape=jax.ShapeDtypeStruct((n_tp, PART_ROWS, tokens * 4), jnp.bfloat16),
        in_specs=[whole(queries.shape)] + [piece(k) for k in range(piece_count)] * len(sources),
        out_specs=whole((n_tp, PART_ROWS, tokens * 4)),
        scratch_shapes=[
            pltpu.VMEM((key_count, 128), jnp.bfloat16),
            pltpu.VMEM((PART_ROWS, key_count), jnp.bfloat16),
            pltpu.VMEM((columns, 128), jnp.bfloat16),
        ],
        cost_estimate=pl.CostEstimate(
            flops=2 * columns * key_count * 512,
            bytes_accessed=2 * key_count * 128,
            transcendentals=columns * key_count,
        ),
        name="attention",
    )(queries, *[source for source in sources for _ in range(piece_count)])


def in_three(matrix):
    high = matrix.astype(jnp.bfloat16)
    rest = matrix - high.astype(jnp.float32)
    middle = rest.astype(jnp.bfloat16)
    return high, middle, (rest - middle.astype(jnp.float32)).astype(jnp.bfloat16)


def recurrence_kernel(raw_ref, leak_ref, extra_ref, local_ref, lifted_ref, sent_ref, held):
    rows, wide = extra_ref.shape
    heads = wide // RECURRENT_WIDTH
    raw_query = raw_ref[:, :wide].astype(jnp.float32)
    raw_gate = raw_ref[:, wide : 2 * wide].astype(jnp.float32)
    query = raw_query * jax.nn.sigmoid(raw_query)
    inflow = leak_ref[...] * (1.0 - jax.nn.sigmoid(raw_gate))
    log_decay = jnp.log(1.0 - inflow) + extra_ref[...]
    lower = lax.broadcasted_iota(jnp.int32, (REC_SPAN, REC_SPAN), 0) >= lax.broadcasted_iota(
        jnp.int32, (REC_SPAN, REC_SPAN), 1
    )
    triangle = jnp.where(lower, 1.0, 0.0).astype(jnp.bfloat16)
    offset = jnp.zeros((1, wide), jnp.float32)
    states = [jnp.zeros((RECURRENT_WIDTH, RECURRENT_WIDTH), jnp.float32)] * heads
    for span in range(rows // REC_SPAN):
        part = slice(span * REC_SPAN, (span + 1) * REC_SPAN)
        running = sum(dot_nn(triangle, term) for term in in_three(log_decay[part]))
        final = running[REC_SPAN - 1 :, :]
        decayed = query[part] * jnp.exp(running)
        lifted = query[part] * jnp.exp(offset + running)
        opened = (inflow[part] * jnp.exp(-running)).astype(jnp.bfloat16)
        closing = (inflow[part] * jnp.exp(final - running)).astype(jnp.bfloat16)
        kept = jnp.exp(final)
        offset = offset + final
        for head in range(heads):
            lanes = slice(head * RECURRENT_WIDTH, (head + 1) * RECURRENT_WIDTH)
            values = raw_ref[part, 2 * wide + lanes.start : 2 * wide + lanes.stop]
            mine = decayed[:, lanes].astype(jnp.bfloat16)
            within = jnp.where(lower, dot_nt(mine, opened[:, lanes]), 0.0)
            local = dot_nn(within.astype(jnp.bfloat16), values)
            if span > 0:
                local = local + dot_nt(mine, states[head].astype(jnp.bfloat16))
            local_ref[head, part, :] = local
            lifted_ref[head, part, :] = lifted[:, lanes].astype(jnp.bfloat16)
            states[head] = kept[:, lanes] * states[head] + lax.dot_general(
                values, closing[:, lanes], (((0,), (0,)), ((), ())),
                preferred_element_type=jnp.float32,
            )
    held[heads * RECURRENT_WIDTH :, :] = jnp.zeros((8, RECURRENT_WIDTH), jnp.float32)
    for head in range(heads):
        held[head * RECURRENT_WIDTH : (head + 1) * RECURRENT_WIDTH, :] = states[head]
    members = sent_ref.shape[0]
    state_row = lax.broadcasted_iota(jnp.int32, (4, RECURRENT_WIDTH), 0) < 2
    decays = jnp.exp(offset)
    for k in range(members):
        head = k * heads // members
        decay = decays[:, head * RECURRENT_WIDTH : (head + 1) * RECURRENT_WIDTH]
        sent_ref[k] = jnp.where(state_row, held[2 * k : 2 * k + 4, :], decay).astype(jnp.bfloat16)


def local_recurrence(raw, leak, extra, members):
    rows, wide = extra.shape
    heads = wide // RECURRENT_WIDTH
    by_head = (heads, rows, RECURRENT_WIDTH)
    sent = (members, 4, RECURRENT_WIDTH)
    return pl.pallas_call(
        recurrence_kernel,
        grid=(1,),
        out_shape=(
            jax.ShapeDtypeStruct(by_head, jnp.float32),
            jax.ShapeDtypeStruct(by_head, jnp.bfloat16),
            jax.ShapeDtypeStruct(sent, jnp.bfloat16),
        ),
        in_specs=[whole(raw.shape), whole(leak.shape), whole(extra.shape)],
        out_specs=(whole(by_head), whole(by_head), whole(sent)),
        scratch_shapes=[pltpu.VMEM((heads * RECURRENT_WIDTH + 8, RECURRENT_WIDTH), jnp.float32)],
        cost_estimate=pl.CostEstimate(
            flops=2 * rows * wide * 1024, bytes_accessed=8 * rows * wide, transcendentals=0
        ),
        name="recurrence",
    )(raw, leak, extra)


def chain_kernel(first_ref, pieces_ref, out_ref):
    def visit(k, state):
        out_ref[k] = state.astype(jnp.bfloat16)
        piece = pieces_ref[k].astype(jnp.float32)
        return piece[2:3, :] * state + piece[0:2, :]

    lax.fori_loop(0, pieces_ref.shape[0], visit, first_ref[...], unroll=8)


def chained(first, pieces):
    count = pieces.shape[0]
    return pl.pallas_call(
        chain_kernel,
        grid=(1,),
        out_shape=jax.ShapeDtypeStruct((count, 2, 128), jnp.bfloat16),
        in_specs=[whole(first.shape), whole(pieces.shape)],
        out_specs=whole((count, 2, 128)),
        name="chained",
    )(first, pieces)


def output_kernel(
    place_ref,
    second_ref,
    parts_ref,
    attn_gain_ref,
    local_ref,
    lifted_ref,
    state_ref,
    rec_gain_ref,
    own_ref,
    other_ref,
    out_ref,
    ordered,
):
    n_lanes = ordered.shape[1]
    first = own_ref.shape[3] - n_lanes
    ordered_rows(place_ref, own_ref, other_ref, slice(first, first + n_lanes), ordered)
    members = parts_ref.shape[0]
    tokens = local_ref.shape[1]
    columns = parts_ref.shape[2]
    half = columns // 2

    def joined(k, row):
        lines = parts_ref[k, HEAD_DIM:, :].astype(jnp.float32)
        return lines[row : row + 1] + lines[row + 1 : row + 2] + lines[row + 2 : row + 3]

    shifts = [joined(k, 3) for k in range(members)]
    top = functools.reduce(jnp.maximum, shifts)
    weighted = jnp.zeros((HEAD_DIM, columns), jnp.float32)
    totals = jnp.zeros((1, columns), jnp.float32)
    for k in range(members):
        factor = jnp.exp2(shifts[k] - top)
        weighted = weighted + parts_ref[k, :HEAD_DIM, :].astype(jnp.float32) * factor
        totals = totals + joined(k, 0) * factor
    ratio = weighted / totals
    head_of = lax.broadcasted_iota(jnp.int32, (1, half), 1) >= tokens
    second = jnp.where(head_of, second_ref[1], second_ref[0])
    blended = ratio[:, :half] - second * ratio[:, half:]
    scale = lax.rsqrt(jnp.mean(blended * blended, axis=0, keepdims=True) + epsilon)
    hidden_t = blended * scale * attn_gain_ref[...]
    turned = jnp.concatenate([hidden_t, hidden_t], axis=0).T
    lane = lax.broadcasted_iota(jnp.int32, (tokens, 2 * HEAD_DIM), 1)
    hidden = [jnp.where(lane < HEAD_DIM, turned[:tokens], turned[tokens:]).astype(jnp.bfloat16)]
    for head in range(local_ref.shape[0]):
        rec = local_ref[head] + dot_nt(lifted_ref[head], state_ref[head])
        scale = lax.rsqrt(jnp.mean(rec * rec, axis=1, keepdims=True) + epsilon)
        hidden.append((rec * scale * rec_gain_ref[...]).astype(jnp.bfloat16))
    hidden = jnp.concatenate(hidden, axis=1)
    step = 512
    for k in range(out_ref.shape[1] // step):
        span = slice(k * step, (k + 1) * step)
        out_ref[:, span] = dot_nt(hidden, ordered[span, :]).astype(jnp.bfloat16)


def output_partial(place, second, parts, attn_gain, local, lifted, state, rec_gain, own, other):
    heads, tokens, width = local.shape
    n_x, n_z, rows, _ = own.shape
    model = n_x * n_z * rows * 2
    mixed = parts.shape[2] // (2 * tokens) * HEAD_DIM + heads * width
    arrays = (parts, attn_gain, local, lifted, state, rec_gain, own, other)
    return pl.pallas_call(
        output_kernel,
        grid=(1,),
        out_shape=jax.ShapeDtypeStruct((tokens, model), jnp.bfloat16),
        in_specs=[in_smem(), in_smem()] + [whole(a.shape) for a in arrays],
        out_specs=whole((tokens, model)),
        scratch_shapes=[pltpu.VMEM((model, mixed), jnp.bfloat16)],
        cost_estimate=pl.CostEstimate(
            flops=2 * tokens * model * mixed, bytes_accessed=2 * model * mixed, transcendentals=0
        ),
        name="output_partial",
    )(place, second, *arrays)


def body(
    tokens,
    input_norm_gain,
    paired_query_weight,
    shared_key_weight,
    shared_value_weight,
    recurrent_query_weight,
    forget_gate_weight,
    recurrent_value_weight,
    attention_output_weight,
    recurrent_output_weight,
    attention_head_gain,
    recurrent_head_gain,
    second_map_weight,
    forget_leak_rate,
    extra_log_decay,
    initial_recurrent_state,
):
    place = jnp.stack([lax.axis_index("c"), lax.axis_index("x")]).astype(jnp.int32)
    own_normed = rms_scale(tokens.astype(jnp.float32), input_norm_gain).astype(jnp.bfloat16)
    own_rows = own_normed.shape[0]
    first_payload = jnp.concatenate(
        [recurrent_query_weight, forget_gate_weight, recurrent_value_weight], axis=1
    )
    key_value = project(
        own_normed, jnp.concatenate([shared_key_weight, shared_value_weight], axis=1)
    )
    rows = paired_query_weight.shape[0]
    narrow = paired_query_weight.shape[1]
    kv_pieces = own_rows // rows
    second_payload = jnp.concatenate(
        [paired_query_weight]
        + [key_value[k * rows : (k + 1) * rows] for k in range(kv_pieces)]
        + [attention_output_weight, recurrent_output_weight],
        axis=1,
    )
    swap = [(0, 1), (1, 0)]
    first_z = sent_to_all(first_payload, "z")
    normed = lax.all_gather(own_normed, "tp", axis=0, tiled=True)
    second_payload, first_z, normed = lax.optimization_barrier((second_payload, first_z, normed))
    second_z = sent_to_all(second_payload, "z")
    first_own = from_others(first_z, "x")
    first_other = lax.ppermute(first_own, "c", swap)
    recur = first_payload.shape[1]
    recur_raw = projections(place, first_own, first_other, normed, recur)
    local_output, lifted, sent = local_recurrence(
        recur_raw, forget_leak_rate[None, :], extra_log_decay, lax.axis_size(SP)
    )
    sent, second_z = lax.optimization_barrier((sent, second_z))
    arrived = lax.all_to_all(sent, SP, 0, 0, tiled=True)
    second_own = from_others(second_z, "x")
    second_other = lax.ppermute(second_own, "c", swap)
    first = lax.dynamic_index_in_dim(
        initial_recurrent_state.transpose(0, 2, 1).reshape(sent.shape[0], 2, 128),
        lax.axis_index(SP),
        0,
        False,
    )
    before = chained(first, arrived)
    incoming_state = lax.all_to_all(before, SP, 0, 0, tiled=True)
    incoming_state = incoming_state.reshape(initial_recurrent_state.shape)
    queries = projections(place, second_own, second_other, normed, narrow)
    all_queries = lax.all_gather(queries, "tp", axis=0)
    parts = attention(all_queries, (second_own, second_other), narrow // 128, kv_pieces)
    landed_parts = lax.all_to_all(parts, "tp", 0, 0, tiled=True)
    partial = output_partial(
        place,
        second_map_weight,
        landed_parts,
        attention_head_gain[:, None],
        local_output,
        lifted,
        incoming_state,
        recurrent_head_gain[None, :],
        second_own,
        second_other,
    )
    size = lax.axis_size("tp")
    blocks = partial.reshape(size, own_rows, partial.shape[1])
    landed = lax.all_to_all(blocks, "tp", 0, 0, tiled=True)
    return landed.astype(jnp.float32).sum(axis=0).astype(jnp.bfloat16)


def solution(mesh):
    torus = Mesh(mesh.devices.reshape(16, 4, 2, mesh.shape["tp"]), SP_TP)
    placed = (
        P(SP_TP, None),
        P(),
        P(SP, "tp"),
        P(),
        P(),
        P(SP, "tp"),
        P(SP, "tp"),
        P(SP, "tp"),
        P(SP, "tp"),
        P(SP, "tp"),
        P(),
        P(),
        P("tp"),
        P("tp"),
        P(SP, "tp"),
        P("tp", None, None),
    )

    return jax.shard_map(
        body, mesh=torus, in_specs=placed, out_specs=P(SP_TP, None), check_vma=False
    )
```

```python
import functools
import math

import jax
import jax.numpy as jnp
from jax import lax
from jax.experimental import pallas as pl
from jax.experimental.pallas import tpu as pltpu
from jax.sharding import Mesh
from jax.sharding import PartitionSpec as P


QK_DIM = 32
HEAD_DIM = 64
RECURRENT_WIDTH = 128
REC_SPAN = 64
SP = ("z", "x", "c")
SP_TP = ("z", "x", "c", "tp")
KEY_BLOCK = 512
COLUMN_TILE = 256
PART_ROWS = 80

epsilon = 1e-06


def sent_to_all(x, axis):
    size = lax.axis_size(axis)
    return lax.all_to_all(jnp.broadcast_to(x[None], (size, *x.shape)), axis, 0, 0, tiled=True)


def from_others(x, axis):
    size = lax.axis_size(axis)
    pieces = [x] + [
        lax.ppermute(x, axis, [((k + ahead) % size, k) for k in range(size)])
        for ahead in range(1, size)
    ]
    return jnp.stack(pieces)


def rms_scale(matrix, gain):
    return matrix * lax.rsqrt(jnp.mean(matrix * matrix, axis=-1, keepdims=True) + epsilon) * gain


def project(normed, weight):
    return jnp.dot(normed, weight, preferred_element_type=jnp.float32).astype(jnp.bfloat16)


def whole(shape):
    return pl.BlockSpec(shape, lambda *_: (0,) * len(shape))


def dot_nt(a, b):
    return lax.dot_general(a, b, (((1,), (1,)), ((), ())), preferred_element_type=jnp.float32)


def dot_nn(a, b):
    return jnp.dot(a, b, preferred_element_type=jnp.float32)


def ordered_rows(place_ref, own_ref, other_ref, lanes, ordered):
    n_x, n_z, rows = own_ref.shape[:3]
    core = place_ref[0]
    for x in range(n_x):
        owner = lax.rem(place_ref[1] + x, n_x)
        for z in range(n_z):
            start = (z * n_x + owner) * 2 * rows
            mine = pl.multiple_of(start + core * rows, rows)
            others = pl.multiple_of(start + (1 - core) * rows, rows)
            ordered[pl.ds(mine, rows), :] = own_ref[x, z, :, lanes]
            ordered[pl.ds(others, rows), :] = other_ref[x, z, :, lanes]


def projection_kernel(place_ref, own_ref, other_ref, normed_ref, out_ref, ordered):
    wide = out_ref.shape[1]
    ordered_rows(place_ref, own_ref, other_ref, slice(0, wide), ordered)
    normed = normed_ref[...]
    step = min(wide, 256)
    for k in range(wide // step):
        span = slice(k * step, (k + 1) * step)
        out_ref[:, span] = dot_nn(normed, ordered[:, span]).astype(jnp.bfloat16)


def in_smem():
    return pl.BlockSpec(memory_space=pltpu.SMEM)


def projections(place, own, other, normed, wide):
    tokens, width = normed.shape
    piece = (*own.shape[:3], wide)
    return pl.pallas_call(
        projection_kernel,
        grid=(1,),
        out_shape=jax.ShapeDtypeStruct((tokens, wide), jnp.bfloat16),
        in_specs=[in_smem(), whole(piece), whole(piece), whole(normed.shape)],
        out_specs=whole((tokens, wide)),
        scratch_shapes=[pltpu.VMEM((width, wide), jnp.bfloat16)],
        cost_estimate=pl.CostEstimate(
            flops=2 * tokens * width * wide, bytes_accessed=2 * width * wide, transcendentals=0
        ),
    )(place, own, other, normed)


def one_hot(rows, cols, row_offset, col_offset, count):
    r = lax.broadcasted_iota(jnp.int32, (rows, cols), 0) - row_offset
    c = lax.broadcasted_iota(jnp.int32, (rows, cols), 1) - col_offset
    hit = (r == c) & (r >= 0) & (r < count)
    return jnp.where(hit, 1.0, 0.0).astype(jnp.bfloat16)


def attention_kernel(query_ref, *refs):
    key_value_refs, (out_ref, keys, values_t, lifted_q) = refs[:-4], refs[-4:]
    n_tp, tokens, _ = query_ref.shape
    n_x, n_z, rows, _ = key_value_refs[0].shape
    piece_rows = n_z * rows
    both = 2 * QK_DIM
    twice = one_hot(128, 128, 0, 0, both) + one_hot(128, 128, 0, both, both)
    pick_values = one_hot(PART_ROWS, 128, 0, both, HEAD_DIM)
    ones_row = jnp.where(
        lax.broadcasted_iota(jnp.int32, (PART_ROWS, piece_rows), 0) == HEAD_DIM, 1.0, 0.0
    )
    key_peak = jnp.zeros((8, 128), jnp.float32)
    index = 0
    for ref in key_value_refs:
        for x in range(n_x):
            piece = ref[x].reshape(piece_rows, 128)
            at = index * piece_rows
            doubled = dot_nn(piece, twice)
            keys[at : at + piece_rows, :] = doubled.astype(jnp.bfloat16)
            size = jnp.abs(doubled).reshape(piece_rows // 8, 8, 128)
            key_peak = jnp.maximum(key_peak, jnp.max(size, axis=0))
            values_t[:, at : at + piece_rows] = (
                dot_nt(pick_values, piece) + ones_row
            ).astype(jnp.bfloat16)
            index += 1
    key_count = index * piece_rows
    scale = math.log2(math.e) / math.sqrt(QK_DIM)
    lane = lax.broadcasted_iota(jnp.int32, (tokens, 128), 1) % both
    for tp in range(n_tp):
        scaled = query_ref[tp].astype(jnp.float32) * scale
        high = scaled.astype(jnp.bfloat16)
        low = (scaled - high.astype(jnp.float32)).astype(jnp.bfloat16)
        for head in range(2):
            spread = dot_nn(high, one_hot(128, 128, head * both, 0, both)) + dot_nn(
                low, one_hot(128, 128, head * both, both, both)
            )
            for part in range(2):
                own = (lane >= part * QK_DIM) & (lane < (part + 1) * QK_DIM)
                at = ((tp * 2 + part) * 2 + head) * tokens
                lifted_q[at : at + tokens, :] = jnp.where(own, spread, 0.0).astype(jnp.bfloat16)
    peak_row = jnp.max(key_peak, axis=0, keepdims=True) * 1.02
    bound = dot_nt(
        jnp.broadcast_to(peak_row, (8, 128)).astype(jnp.bfloat16), jnp.abs(lifted_q[...])
    )
    small = jnp.max(bound) < 100.0
    blocks = key_count // KEY_BLOCK
    tiles = lifted_q.shape[0] // COLUMN_TILE
    per_group = tiles // n_tp

    def store(tile, acc, shift):
        group, place = tile // per_group, tile % per_group
        at = pl.multiple_of(place * COLUMN_TILE, COLUMN_TILE)
        row = lax.broadcasted_iota(jnp.int32, (PART_ROWS - HEAD_DIM, COLUMN_TILE), 0)
        tail = jnp.zeros(row.shape, jnp.float32)
        slot = 0
        for rest in (acc[HEAD_DIM : HEAD_DIM + 1, :], shift):
            for _ in range(3):
                high = rest.astype(jnp.bfloat16).astype(jnp.float32)
                tail = jnp.where(row == slot, high, tail)
                rest = rest - high
                slot += 1
        out_ref[group, :HEAD_DIM, pl.ds(at, COLUMN_TILE)] = acc[:HEAD_DIM, :].astype(jnp.bfloat16)
        out_ref[group, HEAD_DIM:, pl.ds(at, COLUMN_TILE)] = tail.astype(jnp.bfloat16)

    @pl.when(small)
    def _():
        @pl.loop(0, n_tp)
        def _(group):
            first = group * per_group

            def queries_of(place):
                start = pl.multiple_of((first + place) * COLUMN_TILE, COLUMN_TILE)
                return lifted_q[pl.ds(start, COLUMN_TILE), :]

            def scores_of(place, b):
                return dot_nt(keys[b * KEY_BLOCK : (b + 1) * KEY_BLOCK, :], queries_of(place))

            visits = [(place, b) for place in range(per_group) for b in range(blocks)]
            scores = scores_of(*visits[0])
            acc = None
            for turn, (place, b) in enumerate(visits):
                ahead = scores_of(*visits[turn + 1]) if turn + 1 < len(visits) else None
                terms = jnp.exp2(scores).astype(jnp.bfloat16)
                product = dot_nn(values_t[:, b * KEY_BLOCK : (b + 1) * KEY_BLOCK], terms)
                acc = product if b == 0 else acc + product
                if b == blocks - 1:
                    store(first + place, acc, jnp.zeros((1, COLUMN_TILE), jnp.float32))
                scores = ahead

    @pl.when(jnp.logical_not(small))
    def _():
        @pl.loop(0, tiles)
        def _(tile):
            start = pl.multiple_of(tile * COLUMN_TILE, COLUMN_TILE)
            q = lifted_q[pl.ds(start, COLUMN_TILE), :]

            def visit(b, state):
                acc, peak = state
                at = pl.multiple_of(b * KEY_BLOCK, KEY_BLOCK)
                scores = dot_nt(keys[pl.ds(at, KEY_BLOCK), :], q)
                new = jnp.maximum(peak, jnp.max(scores, axis=0, keepdims=True))
                terms = jnp.exp2(scores - new).astype(jnp.bfloat16)
                acc = acc * jnp.exp2(peak - new) + dot_nn(
                    values_t[:, pl.ds(at, KEY_BLOCK)], terms
                )
                return acc, new

            acc, peak = lax.fori_loop(
                0,
                blocks,
                visit,
                (
                    jnp.zeros((PART_ROWS, COLUMN_TILE), jnp.float32),
                    jnp.full((1, COLUMN_TILE), -3e38, jnp.float32),
                ),
            )
            store(tile, acc, peak)


def attention(queries, sources, first_lane_block, piece_count):
    n_tp, tokens, _ = queries.shape
    n_x, n_z, rows, _ = sources[0].shape
    key_count = n_x * n_z * rows * piece_count * len(sources)
    columns = n_tp * tokens * 4

    def piece(k):
        return pl.BlockSpec((n_x, n_z, rows, 128), lambda *_: (0, 0, 0, first_lane_block + k))

    return pl.pallas_call(
        attention_kernel,
        grid=(1,),
        out_shape=jax.ShapeDtypeStruct((n_tp, PART_ROWS, tokens * 4), jnp.bfloat16),
        in_specs=[whole(queries.shape)] + [piece(k) for k in range(piece_count)] * len(sources),
        out_specs=whole((n_tp, PART_ROWS, tokens * 4)),
        scratch_shapes=[
            pltpu.VMEM((key_count, 128), jnp.bfloat16),
            pltpu.VMEM((PART_ROWS, key_count), jnp.bfloat16),
            pltpu.VMEM((columns, 128), jnp.bfloat16),
        ],
        cost_estimate=pl.CostEstimate(
            flops=2 * columns * key_count * 512,
            bytes_accessed=2 * key_count * 128,
            transcendentals=columns * key_count,
        ),
        name="attention",
    )(queries, *[source for source in sources for _ in range(piece_count)])


def in_three(matrix):
    high = matrix.astype(jnp.bfloat16)
    rest = matrix - high.astype(jnp.float32)
    middle = rest.astype(jnp.bfloat16)
    return high, middle, (rest - middle.astype(jnp.float32)).astype(jnp.bfloat16)


def recurrence_kernel(raw_ref, leak_ref, extra_ref, local_ref, lifted_ref, sent_ref, held):
    rows, wide = extra_ref.shape
    heads = wide // RECURRENT_WIDTH
    raw_query = raw_ref[:, :wide].astype(jnp.float32)
    raw_gate = raw_ref[:, wide : 2 * wide].astype(jnp.float32)
    query = raw_query * jax.nn.sigmoid(raw_query)
    inflow = leak_ref[...] * (1.0 - jax.nn.sigmoid(raw_gate))
    log_decay = jnp.log(1.0 - inflow) + extra_ref[...]
    lower = lax.broadcasted_iota(jnp.int32, (REC_SPAN, REC_SPAN), 0) >= lax.broadcasted_iota(
        jnp.int32, (REC_SPAN, REC_SPAN), 1
    )
    triangle = jnp.where(lower, 1.0, 0.0).astype(jnp.bfloat16)
    offset = jnp.zeros((1, wide), jnp.float32)
    states = [jnp.zeros((RECURRENT_WIDTH, RECURRENT_WIDTH), jnp.float32)] * heads
    for span in range(rows // REC_SPAN):
        part = slice(span * REC_SPAN, (span + 1) * REC_SPAN)
        running = sum(dot_nn(triangle, term) for term in in_three(log_decay[part]))
        final = running[REC_SPAN - 1 :, :]
        decayed = query[part] * jnp.exp(running)
        lifted = query[part] * jnp.exp(offset + running)
        opened = (inflow[part] * jnp.exp(-running)).astype(jnp.bfloat16)
        closing = (inflow[part] * jnp.exp(final - running)).astype(jnp.bfloat16)
        kept = jnp.exp(final)
        offset = offset + final
        for head in range(heads):
            lanes = slice(head * RECURRENT_WIDTH, (head + 1) * RECURRENT_WIDTH)
            values = raw_ref[part, 2 * wide + lanes.start : 2 * wide + lanes.stop]
            mine = decayed[:, lanes].astype(jnp.bfloat16)
            within = jnp.where(lower, dot_nt(mine, opened[:, lanes]), 0.0)
            local = dot_nn(within.astype(jnp.bfloat16), values)
            if span > 0:
                local = local + dot_nt(mine, states[head].astype(jnp.bfloat16))
            local_ref[head, part, :] = local
            lifted_ref[head, part, :] = lifted[:, lanes].astype(jnp.bfloat16)
            states[head] = kept[:, lanes] * states[head] + lax.dot_general(
                values, closing[:, lanes], (((0,), (0,)), ((), ())),
                preferred_element_type=jnp.float32,
            )
    held[heads * RECURRENT_WIDTH :, :] = jnp.zeros((8, RECURRENT_WIDTH), jnp.float32)
    for head in range(heads):
        held[head * RECURRENT_WIDTH : (head + 1) * RECURRENT_WIDTH, :] = states[head]
    members = sent_ref.shape[0]
    state_row = lax.broadcasted_iota(jnp.int32, (4, RECURRENT_WIDTH), 0) < 2
    decays = jnp.exp(offset)
    for k in range(members):
        head = k * heads // members
        decay = decays[:, head * RECURRENT_WIDTH : (head + 1) * RECURRENT_WIDTH]
        sent_ref[k] = jnp.where(state_row, held[2 * k : 2 * k + 4, :], decay).astype(jnp.bfloat16)


def local_recurrence(raw, leak, extra, members):
    rows, wide = extra.shape
    heads = wide // RECURRENT_WIDTH
    by_head = (heads, rows, RECURRENT_WIDTH)
    sent = (members, 4, RECURRENT_WIDTH)
    return pl.pallas_call(
        recurrence_kernel,
        grid=(1,),
        out_shape=(
            jax.ShapeDtypeStruct(by_head, jnp.float32),
            jax.ShapeDtypeStruct(by_head, jnp.bfloat16),
            jax.ShapeDtypeStruct(sent, jnp.bfloat16),
        ),
        in_specs=[whole(raw.shape), whole(leak.shape), whole(extra.shape)],
        out_specs=(whole(by_head), whole(by_head), whole(sent)),
        scratch_shapes=[pltpu.VMEM((heads * RECURRENT_WIDTH + 8, RECURRENT_WIDTH), jnp.float32)],
        cost_estimate=pl.CostEstimate(
            flops=2 * rows * wide * 1024, bytes_accessed=8 * rows * wide, transcendentals=0
        ),
        name="recurrence",
    )(raw, leak, extra)


def chain_kernel(first_ref, pieces_ref, out_ref):
    def visit(k, state):
        out_ref[k] = state.astype(jnp.bfloat16)
        piece = pieces_ref[k].astype(jnp.float32)
        return piece[2:3, :] * state + piece[0:2, :]

    lax.fori_loop(0, pieces_ref.shape[0], visit, first_ref[...], unroll=8)


def chained(first, pieces):
    count = pieces.shape[0]
    return pl.pallas_call(
        chain_kernel,
        grid=(1,),
        out_shape=jax.ShapeDtypeStruct((count, 2, 128), jnp.bfloat16),
        in_specs=[whole(first.shape), whole(pieces.shape)],
        out_specs=whole((count, 2, 128)),
        name="chained",
    )(first, pieces)


def output_kernel(
    place_ref,
    second_ref,
    parts_ref,
    attn_gain_ref,
    local_ref,
    lifted_ref,
    state_ref,
    rec_gain_ref,
    own_ref,
    other_ref,
    out_ref,
    ordered,
):
    ordered_rows(place_ref, own_ref, other_ref, slice(0, ordered.shape[1]), ordered)
    members = parts_ref.shape[0]
    tokens = local_ref.shape[1]
    columns = parts_ref.shape[2]
    half = columns // 2

    def joined(k, row):
        lines = parts_ref[k, HEAD_DIM:, :].astype(jnp.float32)
        return lines[row : row + 1] + lines[row + 1 : row + 2] + lines[row + 2 : row + 3]

    shifts = [joined(k, 3) for k in range(members)]
    top = functools.reduce(jnp.maximum, shifts)
    weighted = jnp.zeros((HEAD_DIM, columns), jnp.float32)
    totals = jnp.zeros((1, columns), jnp.float32)
    for k in range(members):
        factor = jnp.exp2(shifts[k] - top)
        weighted = weighted + parts_ref[k, :HEAD_DIM, :].astype(jnp.float32) * factor
        totals = totals + joined(k, 0) * factor
    ratio = weighted / totals
    head_of = lax.broadcasted_iota(jnp.int32, (1, half), 1) >= tokens
    second = jnp.where(head_of, second_ref[1], second_ref[0])
    blended = ratio[:, :half] - second * ratio[:, half:]
    scale = lax.rsqrt(jnp.mean(blended * blended, axis=0, keepdims=True) + epsilon)
    hidden_t = blended * scale * attn_gain_ref[...]
    turned = jnp.concatenate([hidden_t, hidden_t], axis=0).T
    lane = lax.broadcasted_iota(jnp.int32, (tokens, 2 * HEAD_DIM), 1)
    hidden = [jnp.where(lane < HEAD_DIM, turned[:tokens], turned[tokens:]).astype(jnp.bfloat16)]
    for head in range(local_ref.shape[0]):
        rec = local_ref[head] + dot_nt(lifted_ref[head], state_ref[head])
        scale = lax.rsqrt(jnp.mean(rec * rec, axis=1, keepdims=True) + epsilon)
        hidden.append((rec * scale * rec_gain_ref[...]).astype(jnp.bfloat16))
    hidden = jnp.concatenate(hidden, axis=1)
    step = 512
    for k in range(out_ref.shape[1] // step):
        span = slice(k * step, (k + 1) * step)
        out_ref[:, span] = dot_nt(hidden, ordered[span, :]).astype(jnp.bfloat16)


def output_partial(place, second, parts, attn_gain, local, lifted, state, rec_gain, own, other):
    heads, tokens, width = local.shape
    n_x, n_z, rows, lanes = own.shape
    model = n_x * n_z * rows * 2
    mixed = parts.shape[2] // (2 * tokens) * HEAD_DIM + heads * width
    arrays = (parts, attn_gain, local, lifted, state, rec_gain)
    last = pl.BlockSpec((n_x, n_z, rows, mixed), lambda *_: (0, 0, 0, lanes // mixed - 1))
    return pl.pallas_call(
        output_kernel,
        grid=(1,),
        out_shape=jax.ShapeDtypeStruct((tokens, model), jnp.bfloat16),
        in_specs=[in_smem(), in_smem()] + [whole(a.shape) for a in arrays] + [last, last],
        out_specs=whole((tokens, model)),
        scratch_shapes=[pltpu.VMEM((model, mixed), jnp.bfloat16)],
        cost_estimate=pl.CostEstimate(
            flops=2 * tokens * model * mixed, bytes_accessed=2 * model * mixed, transcendentals=0
        ),
        name="output_partial",
    )(place, second, *arrays, own, other)


def body(
    tokens,
    input_norm_gain,
    paired_query_weight,
    shared_key_weight,
    shared_value_weight,
    recurrent_query_weight,
    forget_gate_weight,
    recurrent_value_weight,
    attention_output_weight,
    recurrent_output_weight,
    attention_head_gain,
    recurrent_head_gain,
    second_map_weight,
    forget_leak_rate,
    extra_log_decay,
    initial_recurrent_state,
):
    place = jnp.stack([lax.axis_index("c"), lax.axis_index("x")]).astype(jnp.int32)
    own_normed = rms_scale(tokens.astype(jnp.float32), input_norm_gain).astype(jnp.bfloat16)
    own_rows = own_normed.shape[0]
    key_value = project(
        own_normed, jnp.concatenate([shared_key_weight, shared_value_weight], axis=1)
    )
    rows = paired_query_weight.shape[0]
    narrow = paired_query_weight.shape[1]
    kv_pieces = own_rows // rows
    first_payload = jnp.concatenate(
        [paired_query_weight]
        + [key_value[k * rows : (k + 1) * rows] for k in range(kv_pieces)],
        axis=1,
    )
    recurrence_weights = (recurrent_query_weight, forget_gate_weight, recurrent_value_weight)
    recur = sum(weight.shape[1] for weight in recurrence_weights)
    second_payload = jnp.concatenate(
        [*recurrence_weights, attention_output_weight, recurrent_output_weight], axis=1
    )
    swap = [(0, 1), (1, 0)]
    first_z = sent_to_all(first_payload, "z")
    normed = lax.all_gather(own_normed, "tp", axis=0, tiled=True)
    second_payload, first_z, normed = lax.optimization_barrier((second_payload, first_z, normed))
    second_z = sent_to_all(second_payload, "z")
    first_own = from_others(first_z, "x")
    first_other = lax.ppermute(first_own, "c", swap)
    queries = projections(place, first_own, first_other, normed, narrow)
    all_queries = lax.all_gather(queries, "tp", axis=0)
    all_queries, second_z = lax.optimization_barrier((all_queries, second_z))
    second_own = from_others(second_z, "x")
    parts = attention(all_queries, (first_own, first_other), narrow // 128, kv_pieces)
    landed_parts = lax.all_to_all(parts, "tp", 0, 0, tiled=True)
    second_other = lax.ppermute(second_own, "c", swap)
    recur_raw = projections(place, second_own, second_other, normed, recur)
    local_output, lifted, sent = local_recurrence(
        recur_raw, forget_leak_rate[None, :], extra_log_decay, lax.axis_size(SP)
    )
    arrived = lax.all_to_all(sent, SP, 0, 0, tiled=True)
    first = lax.dynamic_index_in_dim(
        initial_recurrent_state.transpose(0, 2, 1).reshape(sent.shape[0], 2, 128),
        lax.axis_index(SP),
        0,
        False,
    )
    before = chained(first, arrived)
    incoming_state = lax.all_to_all(before, SP, 0, 0, tiled=True)
    incoming_state = incoming_state.reshape(initial_recurrent_state.shape)
    partial = output_partial(
        place,
        second_map_weight,
        landed_parts,
        attention_head_gain[:, None],
        local_output,
        lifted,
        incoming_state,
        recurrent_head_gain[None, :],
        second_own,
        second_other,
    )
    size = lax.axis_size("tp")
    blocks = partial.reshape(size, own_rows, partial.shape[1])
    landed = lax.all_to_all(blocks, "tp", 0, 0, tiled=True)
    return landed.astype(jnp.float32).sum(axis=0).astype(jnp.bfloat16)


def solution(mesh):
    torus = Mesh(mesh.devices.reshape(16, 4, 2, mesh.shape["tp"]), SP_TP)
    placed = (
        P(SP_TP, None),
        P(),
        P(SP, "tp"),
        P(),
        P(),
        P(SP, "tp"),
        P(SP, "tp"),
        P(SP, "tp"),
        P(SP, "tp"),
        P(SP, "tp"),
        P(),
        P(),
        P("tp"),
        P("tp"),
        P(SP, "tp"),
        P("tp", None, None),
    )

    return jax.shard_map(
        body, mesh=torus, in_specs=placed, out_specs=P(SP_TP, None), check_vma=False
    )
```

```python
import functools
import math

import jax
import jax.numpy as jnp
from jax import lax
from jax.experimental import pallas as pl
from jax.experimental.pallas import tpu as pltpu
from jax.sharding import Mesh
from jax.sharding import PartitionSpec as P


QK_DIM = 32
HEAD_DIM = 64
RECURRENT_WIDTH = 128
REC_SPAN = 64
SP = ("z", "x", "c")
PLANE = ("x", "c")
SP_TP = ("z", "x", "c", "tp")
KEY_BLOCK = 512
COLUMN_TILE = 256
PART_ROWS = 80
DECAY_ROWS = 16

epsilon = 1e-06


def sent_to_all(x, axis):
    size = lax.axis_size(axis)
    return lax.all_to_all(jnp.broadcast_to(x[None], (size, *x.shape)), axis, 0, 0, tiled=True)


def from_others(x, axis):
    size = lax.axis_size(axis)
    pieces = [x] + [
        lax.ppermute(x, axis, [((k + ahead) % size, k) for k in range(size)])
        for ahead in range(1, size)
    ]
    return jnp.stack(pieces)


def rms_scale(matrix, gain):
    return matrix * lax.rsqrt(jnp.mean(matrix * matrix, axis=-1, keepdims=True) + epsilon) * gain


def project(normed, weight):
    return jnp.dot(normed, weight, preferred_element_type=jnp.float32).astype(jnp.bfloat16)


def whole(shape):
    return pl.BlockSpec(shape, lambda *_: (0,) * len(shape))


def dot_nt(a, b):
    return lax.dot_general(a, b, (((1,), (1,)), ((), ())), preferred_element_type=jnp.float32)


def dot_nn(a, b):
    return jnp.dot(a, b, preferred_element_type=jnp.float32)


def ordered_rows(place_ref, own_ref, other_ref, lanes, ordered, from_own):
    n_x, n_z, rows = own_ref.shape[:3]
    core = place_ref[0]
    for x in range(n_x):
        owner = lax.rem(place_ref[1] + x, n_x) if from_own else x
        for z in range(n_z):
            start = (z * n_x + owner) * 2 * rows
            mine = pl.multiple_of(start + core * rows, rows)
            others = pl.multiple_of(start + (1 - core) * rows, rows)
            ordered[pl.ds(mine, rows), :] = own_ref[x, z, :, lanes]
            ordered[pl.ds(others, rows), :] = other_ref[x, z, :, lanes]


def projection_kernel(from_own, place_ref, own_ref, other_ref, normed_ref, out_ref, ordered):
    wide = out_ref.shape[1]
    ordered_rows(place_ref, own_ref, other_ref, slice(0, wide), ordered, from_own)
    normed = normed_ref[...]
    step = min(wide, 256)
    for k in range(wide // step):
        span = slice(k * step, (k + 1) * step)
        out_ref[:, span] = dot_nn(normed, ordered[:, span]).astype(jnp.bfloat16)


def in_smem():
    return pl.BlockSpec(memory_space=pltpu.SMEM)


def projections(place, own, other, normed, wide, from_own):
    tokens, width = normed.shape
    piece = (*own.shape[:3], wide)
    return pl.pallas_call(
        functools.partial(projection_kernel, from_own),
        grid=(1,),
        out_shape=jax.ShapeDtypeStruct((tokens, wide), jnp.bfloat16),
        in_specs=[in_smem(), whole(piece), whole(piece), whole(normed.shape)],
        out_specs=whole((tokens, wide)),
        scratch_shapes=[pltpu.VMEM((width, wide), jnp.bfloat16)],
        cost_estimate=pl.CostEstimate(
            flops=2 * tokens * width * wide, bytes_accessed=2 * width * wide, transcendentals=0
        ),
    )(place, own, other, normed)


def one_hot(rows, cols, row_offset, col_offset, count):
    r = lax.broadcasted_iota(jnp.int32, (rows, cols), 0) - row_offset
    c = lax.broadcasted_iota(jnp.int32, (rows, cols), 1) - col_offset
    hit = (r == c) & (r >= 0) & (r < count)
    return jnp.where(hit, 1.0, 0.0).astype(jnp.bfloat16)


def attention_kernel(query_ref, *refs):
    key_value_refs, (out_ref, keys, values_t, lifted_q) = refs[:-4], refs[-4:]
    n_tp, tokens, _ = query_ref.shape
    n_x, n_z, rows, _ = key_value_refs[0].shape
    piece_rows = n_z * rows
    both = 2 * QK_DIM
    twice = one_hot(128, 128, 0, 0, both) + one_hot(128, 128, 0, both, both)
    pick_values = one_hot(PART_ROWS, 128, 0, both, HEAD_DIM)
    ones_row = jnp.where(
        lax.broadcasted_iota(jnp.int32, (PART_ROWS, piece_rows), 0) == HEAD_DIM, 1.0, 0.0
    )
    key_peak = jnp.zeros((8, 128), jnp.float32)
    index = 0
    for ref in key_value_refs:
        for x in range(n_x):
            piece = ref[x].reshape(piece_rows, 128)
            at = index * piece_rows
            doubled = dot_nn(piece, twice)
            keys[at : at + piece_rows, :] = doubled.astype(jnp.bfloat16)
            size = jnp.abs(doubled).reshape(piece_rows // 8, 8, 128)
            key_peak = jnp.maximum(key_peak, jnp.max(size, axis=0))
            values_t[:, at : at + piece_rows] = (
                dot_nt(pick_values, piece) + ones_row
            ).astype(jnp.bfloat16)
            index += 1
    key_count = index * piece_rows
    scale = math.log2(math.e) / math.sqrt(QK_DIM)
    lane = lax.broadcasted_iota(jnp.int32, (tokens, 128), 1) % both
    for tp in range(n_tp):
        scaled = query_ref[tp].astype(jnp.float32) * scale
        high = scaled.astype(jnp.bfloat16)
        low = (scaled - high.astype(jnp.float32)).astype(jnp.bfloat16)
        for head in range(2):
            spread = dot_nn(high, one_hot(128, 128, head * both, 0, both)) + dot_nn(
                low, one_hot(128, 128, head * both, both, both)
            )
            for part in range(2):
                own = (lane >= part * QK_DIM) & (lane < (part + 1) * QK_DIM)
                at = ((tp * 2 + part) * 2 + head) * tokens
                lifted_q[at : at + tokens, :] = jnp.where(own, spread, 0.0).astype(jnp.bfloat16)
    peak_row = jnp.max(key_peak, axis=0, keepdims=True) * 1.02
    bound = dot_nt(
        jnp.broadcast_to(peak_row, (8, 128)).astype(jnp.bfloat16), jnp.abs(lifted_q[...])
    )
    small = jnp.max(bound) < 100.0
    blocks = key_count // KEY_BLOCK
    tiles = lifted_q.shape[0] // COLUMN_TILE
    per_group = tiles // n_tp

    def store(tile, acc, shift):
        group, place = tile // per_group, tile % per_group
        at = pl.multiple_of(place * COLUMN_TILE, COLUMN_TILE)
        row = lax.broadcasted_iota(jnp.int32, (PART_ROWS - HEAD_DIM, COLUMN_TILE), 0)
        tail = jnp.zeros(row.shape, jnp.float32)
        slot = 0
        for rest in (acc[HEAD_DIM : HEAD_DIM + 1, :], shift):
            for _ in range(3):
                high = rest.astype(jnp.bfloat16).astype(jnp.float32)
                tail = jnp.where(row == slot, high, tail)
                rest = rest - high
                slot += 1
        out_ref[group, :HEAD_DIM, pl.ds(at, COLUMN_TILE)] = acc[:HEAD_DIM, :].astype(jnp.bfloat16)
        out_ref[group, HEAD_DIM:, pl.ds(at, COLUMN_TILE)] = tail.astype(jnp.bfloat16)

    @pl.when(small)
    def _():
        @pl.loop(0, n_tp)
        def _(group):
            first = group * per_group

            def queries_of(place):
                start = pl.multiple_of((first + place) * COLUMN_TILE, COLUMN_TILE)
                return lifted_q[pl.ds(start, COLUMN_TILE), :]

            def scores_of(place, b):
                return dot_nt(keys[b * KEY_BLOCK : (b + 1) * KEY_BLOCK, :], queries_of(place))

            visits = [(place, b) for place in range(per_group) for b in range(blocks)]
            scores = scores_of(*visits[0])
            acc = None
            for turn, (place, b) in enumerate(visits):
                ahead = scores_of(*visits[turn + 1]) if turn + 1 < len(visits) else None
                terms = jnp.exp2(scores).astype(jnp.bfloat16)
                product = dot_nn(values_t[:, b * KEY_BLOCK : (b + 1) * KEY_BLOCK], terms)
                acc = product if b == 0 else acc + product
                if b == blocks - 1:
                    store(first + place, acc, jnp.zeros((1, COLUMN_TILE), jnp.float32))
                scores = ahead

    @pl.when(jnp.logical_not(small))
    def _():
        @pl.loop(0, tiles)
        def _(tile):
            start = pl.multiple_of(tile * COLUMN_TILE, COLUMN_TILE)
            q = lifted_q[pl.ds(start, COLUMN_TILE), :]

            def visit(b, state):
                acc, peak = state
                at = pl.multiple_of(b * KEY_BLOCK, KEY_BLOCK)
                scores = dot_nt(keys[pl.ds(at, KEY_BLOCK), :], q)
                new = jnp.maximum(peak, jnp.max(scores, axis=0, keepdims=True))
                terms = jnp.exp2(scores - new).astype(jnp.bfloat16)
                acc = acc * jnp.exp2(peak - new) + dot_nn(
                    values_t[:, pl.ds(at, KEY_BLOCK)], terms
                )
                return acc, new

            acc, peak = lax.fori_loop(
                0,
                blocks,
                visit,
                (
                    jnp.zeros((PART_ROWS, COLUMN_TILE), jnp.float32),
                    jnp.full((1, COLUMN_TILE), -3e38, jnp.float32),
                ),
            )
            store(tile, acc, peak)


def attention(queries, sources, first_lane_block, piece_count):
    n_tp, tokens, _ = queries.shape
    n_x, n_z, rows, _ = sources[0].shape
    key_count = n_x * n_z * rows * piece_count * len(sources)
    columns = n_tp * tokens * 4

    def piece(k):
        return pl.BlockSpec((n_x, n_z, rows, 128), lambda *_: (0, 0, 0, first_lane_block + k))

    return pl.pallas_call(
        attention_kernel,
        grid=(1,),
        out_shape=jax.ShapeDtypeStruct((n_tp, PART_ROWS, tokens * 4), jnp.bfloat16),
        in_specs=[whole(queries.shape)] + [piece(k) for k in range(piece_count)] * len(sources),
        out_specs=whole((n_tp, PART_ROWS, tokens * 4)),
        scratch_shapes=[
            pltpu.VMEM((key_count, 128), jnp.bfloat16),
            pltpu.VMEM((PART_ROWS, key_count), jnp.bfloat16),
            pltpu.VMEM((columns, 128), jnp.bfloat16),
        ],
        cost_estimate=pl.CostEstimate(
            flops=2 * columns * key_count * 512,
            bytes_accessed=2 * key_count * 128,
            transcendentals=columns * key_count,
        ),
        name="attention",
    )(queries, *[source for source in sources for _ in range(piece_count)])


def in_three(matrix):
    high = matrix.astype(jnp.bfloat16)
    rest = matrix - high.astype(jnp.float32)
    middle = rest.astype(jnp.bfloat16)
    return high, middle, (rest - middle.astype(jnp.float32)).astype(jnp.bfloat16)


def recurrence_kernel(raw_ref, leak_ref, extra_ref, local_ref, lifted_ref, sent_ref):
    rows, wide = extra_ref.shape
    heads = wide // RECURRENT_WIDTH
    raw_query = raw_ref[:, :wide].astype(jnp.float32)
    raw_gate = raw_ref[:, wide : 2 * wide].astype(jnp.float32)
    query = raw_query * jax.nn.sigmoid(raw_query)
    inflow = leak_ref[...] * (1.0 - jax.nn.sigmoid(raw_gate))
    log_decay = jnp.log(1.0 - inflow) + extra_ref[...]
    lower = lax.broadcasted_iota(jnp.int32, (REC_SPAN, REC_SPAN), 0) >= lax.broadcasted_iota(
        jnp.int32, (REC_SPAN, REC_SPAN), 1
    )
    triangle = jnp.where(lower, 1.0, 0.0).astype(jnp.bfloat16)
    offset = jnp.zeros((1, wide), jnp.float32)
    states = [jnp.zeros((RECURRENT_WIDTH, RECURRENT_WIDTH), jnp.float32)] * heads
    for span in range(rows // REC_SPAN):
        part = slice(span * REC_SPAN, (span + 1) * REC_SPAN)
        running = sum(dot_nn(triangle, term) for term in in_three(log_decay[part]))
        final = running[REC_SPAN - 1 :, :]
        decayed = query[part] * jnp.exp(running)
        lifted = query[part] * jnp.exp(offset + running)
        opened = (inflow[part] * jnp.exp(-running)).astype(jnp.bfloat16)
        closing = (inflow[part] * jnp.exp(final - running)).astype(jnp.bfloat16)
        kept = jnp.exp(final)
        offset = offset + final
        for head in range(heads):
            lanes = slice(head * RECURRENT_WIDTH, (head + 1) * RECURRENT_WIDTH)
            values = raw_ref[part, 2 * wide + lanes.start : 2 * wide + lanes.stop]
            mine = decayed[:, lanes].astype(jnp.bfloat16)
            within = jnp.where(lower, dot_nt(mine, opened[:, lanes]), 0.0)
            local = dot_nn(within.astype(jnp.bfloat16), values)
            if span > 0:
                local = local + dot_nt(mine, states[head].astype(jnp.bfloat16))
            local_ref[head, part, :] = local
            lifted_ref[head, part, :] = lifted[:, lanes].astype(jnp.bfloat16)
            states[head] = kept[:, lanes] * states[head] + lax.dot_general(
                values, closing[:, lanes], (((0,), (0,)), ((), ())),
                preferred_element_type=jnp.float32,
            )
    members, piece_rows, _ = sent_ref.shape
    share = heads * RECURRENT_WIDTH // members
    decays = jnp.exp(offset)
    for k in range(members):
        head, start = k * share // RECURRENT_WIDTH, k * share % RECURRENT_WIDTH
        decay = decays[:, head * RECURRENT_WIDTH : (head + 1) * RECURRENT_WIDTH]
        sent_ref[k, :share, :] = states[head][start : start + share].astype(jnp.bfloat16)
        sent_ref[k, share:, :] = jnp.broadcast_to(
            decay, (piece_rows - share, RECURRENT_WIDTH)
        ).astype(jnp.bfloat16)


def local_recurrence(raw, leak, extra, members):
    rows, wide = extra.shape
    heads = wide // RECURRENT_WIDTH
    by_head = (heads, rows, RECURRENT_WIDTH)
    sent = (members, heads * RECURRENT_WIDTH // members + DECAY_ROWS, RECURRENT_WIDTH)
    return pl.pallas_call(
        recurrence_kernel,
        grid=(1,),
        out_shape=(
            jax.ShapeDtypeStruct(by_head, jnp.float32),
            jax.ShapeDtypeStruct(by_head, jnp.bfloat16),
            jax.ShapeDtypeStruct(sent, jnp.bfloat16),
        ),
        in_specs=[whole(raw.shape), whole(leak.shape), whole(extra.shape)],
        out_specs=(whole(by_head), whole(by_head), whole(sent)),
        cost_estimate=pl.CostEstimate(
            flops=2 * rows * wide * 1024, bytes_accessed=8 * rows * wide, transcendentals=0
        ),
        name="recurrence",
    )(raw, leak, extra)


def passed(pieces_ref, k, state, share):
    decay = pieces_ref[k, share : share + 1, :].astype(jnp.float32)
    return decay * state + pieces_ref[k, :share, :].astype(jnp.float32), decay


def plane_kernel(pieces_ref, out_ref):
    members, piece_rows, width = pieces_ref.shape
    share = piece_rows - DECAY_ROWS
    state = jnp.zeros((share, width), jnp.float32)
    total = jnp.ones((1, width), jnp.float32)
    for k in range(members):
        state, decay = passed(pieces_ref, k, state, share)
        total = total * decay
    state = state.astype(jnp.bfloat16)
    total = jnp.broadcast_to(total, (DECAY_ROWS, width)).astype(jnp.bfloat16)
    for k in range(out_ref.shape[0]):
        out_ref[k, :share, :] = state
        out_ref[k, share:, :] = total


def before_kernel(place_ref, first_ref, planes_ref, pieces_ref, out_ref):
    members, share, _ = out_ref.shape
    mine = place_ref[1] * 2 + place_ref[0]
    state = lax.fori_loop(
        0,
        place_ref[2],
        lambda k, state: passed(planes_ref, k, state, share)[0],
        first_ref[mine],
    )
    for k in range(members):
        out_ref[k] = state.astype(jnp.bfloat16)
        state, _ = passed(pieces_ref, k, state, share)


def plane_total(pieces, planes):
    out = (planes, *pieces.shape[1:])
    return pl.pallas_call(
        plane_kernel,
        grid=(1,),
        out_shape=jax.ShapeDtypeStruct(out, jnp.bfloat16),
        in_specs=[whole(pieces.shape)],
        out_specs=whole(out),
        name="plane_total",
    )(pieces)


def states_before(place, first, planes, pieces):
    arrays = (first, planes, pieces)
    return pl.pallas_call(
        before_kernel,
        grid=(1,),
        out_shape=jax.ShapeDtypeStruct(first.shape, jnp.bfloat16),
        in_specs=[in_smem()] + [whole(a.shape) for a in arrays],
        out_specs=whole(first.shape),
        name="states_before",
    )(place, *arrays)


def output_kernel(
    place_ref,
    second_ref,
    parts_ref,
    attn_gain_ref,
    local_ref,
    lifted_ref,
    state_ref,
    rec_gain_ref,
    own_ref,
    other_ref,
    out_ref,
    ordered,
):
    ordered_rows(place_ref, own_ref, other_ref, slice(0, ordered.shape[1]), ordered, False)
    members = parts_ref.shape[0]
    tokens = local_ref.shape[1]
    columns = parts_ref.shape[2]
    half = columns // 2

    def joined(k, row):
        lines = parts_ref[k, HEAD_DIM:, :].astype(jnp.float32)
        return lines[row : row + 1] + lines[row + 1 : row + 2] + lines[row + 2 : row + 3]

    shifts = [joined(k, 3) for k in range(members)]
    top = functools.reduce(jnp.maximum, shifts)
    weighted = jnp.zeros((HEAD_DIM, columns), jnp.float32)
    totals = jnp.zeros((1, columns), jnp.float32)
    for k in range(members):
        factor = jnp.exp2(shifts[k] - top)
        weighted = weighted + parts_ref[k, :HEAD_DIM, :].astype(jnp.float32) * factor
        totals = totals + joined(k, 0) * factor
    ratio = weighted / totals
    head_of = lax.broadcasted_iota(jnp.int32, (1, half), 1) >= tokens
    second = jnp.where(head_of, second_ref[1], second_ref[0])
    blended = ratio[:, :half] - second * ratio[:, half:]
    scale = lax.rsqrt(jnp.mean(blended * blended, axis=0, keepdims=True) + epsilon)
    hidden_t = blended * scale * attn_gain_ref[...]
    turned = jnp.concatenate([hidden_t, hidden_t], axis=0).T
    lane = lax.broadcasted_iota(jnp.int32, (tokens, 2 * HEAD_DIM), 1)
    hidden = [jnp.where(lane < HEAD_DIM, turned[:tokens], turned[tokens:]).astype(jnp.bfloat16)]
    for head in range(local_ref.shape[0]):
        rec = local_ref[head] + dot_nt(lifted_ref[head], state_ref[head])
        scale = lax.rsqrt(jnp.mean(rec * rec, axis=1, keepdims=True) + epsilon)
        hidden.append((rec * scale * rec_gain_ref[...]).astype(jnp.bfloat16))
    hidden = jnp.concatenate(hidden, axis=1)
    step = 512
    for k in range(out_ref.shape[1] // step):
        span = slice(k * step, (k + 1) * step)
        out_ref[:, span] = dot_nt(hidden, ordered[span, :]).astype(jnp.bfloat16)


def output_partial(place, second, parts, attn_gain, local, lifted, state, rec_gain, own, other):
    heads, tokens, width = local.shape
    n_x, n_z, rows, lanes = own.shape
    model = n_x * n_z * rows * 2
    mixed = parts.shape[2] // (2 * tokens) * HEAD_DIM + heads * width
    arrays = (parts, attn_gain, local, lifted, state, rec_gain)
    last = pl.BlockSpec((n_x, n_z, rows, mixed), lambda *_: (0, 0, 0, lanes // mixed - 1))
    return pl.pallas_call(
        output_kernel,
        grid=(1,),
        out_shape=jax.ShapeDtypeStruct((tokens, model), jnp.bfloat16),
        in_specs=[in_smem(), in_smem()] + [whole(a.shape) for a in arrays] + [last, last],
        out_specs=whole((tokens, model)),
        scratch_shapes=[pltpu.VMEM((model, mixed), jnp.bfloat16)],
        cost_estimate=pl.CostEstimate(
            flops=2 * tokens * model * mixed, bytes_accessed=2 * model * mixed, transcendentals=0
        ),
        name="output_partial",
    )(place, second, *arrays, own, other)


def body(
    tokens,
    input_norm_gain,
    paired_query_weight,
    shared_key_weight,
    shared_value_weight,
    recurrent_query_weight,
    forget_gate_weight,
    recurrent_value_weight,
    attention_output_weight,
    recurrent_output_weight,
    attention_head_gain,
    recurrent_head_gain,
    second_map_weight,
    forget_leak_rate,
    extra_log_decay,
    initial_recurrent_state,
):
    place = jnp.stack([lax.axis_index(axis) for axis in ("c", "x", "z")]).astype(jnp.int32)
    own_normed = rms_scale(tokens.astype(jnp.float32), input_norm_gain).astype(jnp.bfloat16)
    own_rows = own_normed.shape[0]
    key_value = project(
        own_normed, jnp.concatenate([shared_key_weight, shared_value_weight], axis=1)
    )
    rows = paired_query_weight.shape[0]
    narrow = paired_query_weight.shape[1]
    kv_pieces = own_rows // rows
    first_payload = jnp.concatenate(
        [paired_query_weight]
        + [key_value[k * rows : (k + 1) * rows] for k in range(kv_pieces)],
        axis=1,
    )
    recurrence_weights = (recurrent_query_weight, forget_gate_weight, recurrent_value_weight)
    recur = sum(weight.shape[1] for weight in recurrence_weights)
    second_payload = jnp.concatenate(
        [*recurrence_weights, attention_output_weight, recurrent_output_weight], axis=1
    )
    swap = [(0, 1), (1, 0)]
    first_z = sent_to_all(first_payload, "z")
    normed = lax.all_gather(own_normed, "tp", axis=0, tiled=True)
    second_payload, first_z, normed = lax.optimization_barrier((second_payload, first_z, normed))
    second_z = sent_to_all(second_payload, "z")
    first_own = from_others(first_z, "x")
    first_other = lax.ppermute(first_own, "c", swap)
    queries = projections(place, first_own, first_other, normed, narrow, True)
    all_queries = lax.all_gather(queries, "tp", axis=0)
    all_queries, second_z = lax.optimization_barrier((all_queries, second_z))
    second_own = sent_to_all(second_z, "x")
    parts = attention(all_queries, (first_own, first_other), narrow // 128, kv_pieces)
    landed_parts = lax.all_to_all(parts, "tp", 0, 0, tiled=True)
    second_other = lax.ppermute(second_own, "c", swap)
    recur_raw = projections(place, second_own, second_other, normed, recur, False)
    members = lax.axis_size(PLANE)
    local_output, lifted, sent = local_recurrence(
        recur_raw, forget_leak_rate[None, :], extra_log_decay, members
    )
    pieces = lax.all_to_all(sent, PLANE, 0, 0, tiled=True)
    total = plane_total(pieces, lax.axis_size("z"))
    planes = lax.all_to_all(total, "z", 0, 0, tiled=True)
    first = initial_recurrent_state.transpose(0, 2, 1).reshape(members, -1, RECURRENT_WIDTH)
    before = states_before(place, first, planes, pieces)
    incoming_state = lax.all_to_all(before, PLANE, 0, 0, tiled=True)
    incoming_state = incoming_state.reshape(initial_recurrent_state.shape)
    partial = output_partial(
        place,
        second_map_weight,
        landed_parts,
        attention_head_gain[:, None],
        local_output,
        lifted,
        incoming_state,
        recurrent_head_gain[None, :],
        second_own,
        second_other,
    )
    size = lax.axis_size("tp")
    blocks = partial.reshape(size, own_rows, partial.shape[1])
    landed = lax.all_to_all(blocks, "tp", 0, 0, tiled=True)
    return landed.astype(jnp.float32).sum(axis=0).astype(jnp.bfloat16)


def solution(mesh):
    torus = Mesh(mesh.devices.reshape(16, 4, 2, mesh.shape["tp"]), SP_TP)
    placed = (
        P(SP_TP, None),
        P(),
        P(SP, "tp"),
        P(),
        P(),
        P(SP, "tp"),
        P(SP, "tp"),
        P(SP, "tp"),
        P(SP, "tp"),
        P(SP, "tp"),
        P(),
        P(),
        P("tp"),
        P("tp"),
        P(SP, "tp"),
        P("tp", None, None),
    )

    return jax.shard_map(
        body, mesh=torus, in_specs=placed, out_specs=P(SP_TP, None), check_vma=False
    )
```
